256 devices in a mesh: ep: 128 (over z, y, x), tp: 2 (over core).
Axes of the slice: x: 4, y: 4, z: 8, core: 2. Of those that a mesh axis runs over, the one named last changes fastest.
Arguments:
- tokens_in: bfloat16 [4096, 2048], P('ep'), may hold values from -6 to 6
- state_in: float32 [4096, 8, 64, 64], P('ep', 'tp'), may hold values from -4 to 4
- norm_mix: bfloat16 [2048], replicated, may hold values from 0.099609375 to 1.8984375
- w_recept: bfloat16 [2048, 512], P(None, 'tp'), may hold values from -0.125 to 0.125
- w_key: bfloat16 [2048, 512], P(None, 'tp'), may hold values from -0.125 to 0.125
- w_value: bfloat16 [2048, 512], P(None, 'tp'), may hold values from -0.125 to 0.125
- decay_down: bfloat16 [2048, 64], replicated, may hold values from -0.125 to 0.125
- decay_up: bfloat16 [64, 512], P(None, 'tp'), may hold values from -0.75 to 0.75
- decay_base: float32 [512], P('tp'), may hold values from -4 to 2
- iclr_down: bfloat16 [2048, 64], replicated, may hold values from -0.125 to 0.125
- iclr_up: bfloat16 [64, 512], P(None, 'tp'), may hold values from -0.75 to 0.75
- iclr_base: float32 [512], P('tp'), may hold values from -4 to 4
- key_scale: bfloat16 [512], P('tp'), may hold values from 0.099609375 to 1.8984375
- key_mix: bfloat16 [512], P('tp'), may hold values from 0.099609375 to 1.8984375
- w_out: bfloat16 [512, 2048], P('tp'), may hold values from -0.046875 to 0.046875
- norm_moe: bfloat16 [2048], replicated, may hold values from 0.099609375 to 1.8984375
- router_group: bfloat16 [2048, 16], replicated, may hold values from -0.125 to 0.125
- router_expert: bfloat16 [2048, 128], replicated, may hold values from -0.125 to 0.125
- routes: int32 [4096, 4], P('ep'), may hold values from 0 to 127, as said below
- expert_gate: bfloat16 [128, 2048, 256], P('ep', None, 'tp'), may hold values from -0.125 to 0.125
- expert_up: bfloat16 [128, 2048, 256], P('ep', None, 'tp'), may hold values from -0.125 to 0.125
- expert_down: bfloat16 [128, 256, 2048], P('ep', 'tp'), may hold values from -1.5 to 1.5
Outputs:
- layer_out: bfloat16 [4096, 2048], P('ep', 'tp')
- state_out: float32 [4096, 8, 64, 64], P('ep', 'tp')
The draws below stay inside these ranges and needn't reach their ends.
Inputs may be any that keep to these rules, and one draw needn't show every extreme that they name: `routes`: each row names 4 different experts of one group (the same value of id // 8). Among the rows of one device no expert is named by more than 2 rows, and in every draw one expert is named by exactly 2 rows of every device.
All inputs are finite; a program needn't handle non-finite values.
Results may differ from the reference program's by a relative error of at most 0.018.
Values may be sent and summed in bfloat16 or wider, within the bound.
A program may use at most 64 MiB of HBM per device.

```python
import jax
import jax.numpy as jnp
from jax import lax

D = 2048
HEADS = 8
HEAD = 64
RANK = 64
FE = 256
GROUP_EXPERTS = 8
TOPK = 4
SEQ_DEV = 32
WIDTH = 512
TOKENS = 4096
EXPERTS = 128
GROUPS = 16
CAP = 2
N_EP = 128
N_TP = 2


def draw_routes(key, part):
    base = jax.random.fold_in(key, 7)
    keys = jax.random.split(base, 7)
    blocks = TOKENS // SEQ_DEV
    total_rows = blocks * SEQ_DEV
    hot_group = jax.random.randint(keys[0], (), 0, GROUPS)
    hot_inner = jax.random.randint(keys[1], (), 0, GROUP_EXPERTS)
    order = jax.vmap(lambda sub: jax.random.permutation(sub, SEQ_DEV))(jax.random.split(keys[2], blocks))
    band = order // CAP
    others = jax.vmap(lambda sub: jax.random.permutation(sub, max(GROUPS - 1, 1)))(jax.random.split(keys[3], blocks))
    chosen = jnp.take_along_axis(others, jnp.maximum(band - 1, 0), axis=1)
    group_ids = jnp.where(band == 0, hot_group, (hot_group + 1 + chosen) % GROUPS).reshape(total_rows, 1)
    free_pick = jax.vmap(lambda sub: jax.random.permutation(sub, GROUP_EXPERTS))(jax.random.split(keys[4], total_rows))[:, :TOPK]
    rest = jax.vmap(lambda sub: jax.random.permutation(sub, GROUP_EXPERTS - 1))(jax.random.split(keys[5], total_rows))[:, :TOPK - 1]
    forced = jnp.concatenate([jnp.zeros((total_rows, 1), jnp.int32) + hot_inner, (hot_inner + 1 + rest) % GROUP_EXPERTS], axis=1)
    inner = jnp.where(band.reshape(total_rows, 1) == 0, forced, free_pick)
    column_order = jax.vmap(lambda sub: jax.random.permutation(sub, TOPK))(jax.random.split(keys[6], total_rows))
    inner = jnp.take_along_axis(inner, column_order, axis=1)
    return (group_ids * GROUP_EXPERTS + inner).astype(jnp.int32)


def steps_of(rng, extent, pieces, least, high):
    gain = 1.0
    for dim, parts in pieces:
        draws = jax.random.uniform(jax.random.fold_in(jax.random.fold_in(rng, 6), dim), (parts,), jnp.float32, least / len(pieces), high / len(pieces))
        gain = gain * jnp.repeat(jnp.exp(draws), extent[dim] // parts).reshape((-1,) + (1,) * (len(extent) - 1 - dim))
    return gain


def centred(own_key, shape, scale, reach, shards=(), held_as=jnp.bfloat16):
    values = jax.random.normal(own_key, shape, jnp.float32) * scale
    if len(shards) > 0:
        values = steps_of(own_key, shape, shards, -0.22, 0.18) * values
    return jnp.clip(values, min=-reach, max=reach).astype(held_as)


def setup_inputs(seed: int = 0) -> dict:
    streams_of = jax.random.split(jax.random.key(seed), 23)
    return {
        "tokens_in": centred(streams_of[0], (TOKENS, D), 1.0, 6.0, ((0, 128),)),
        "state_in": centred(streams_of[1], (TOKENS, HEADS, HEAD, HEAD), 0.5, 4.0, ((0, 128), (1, 2)), jnp.float32),
        "norm_mix": jnp.clip(1.0 + 0.18 * jax.random.normal(streams_of[2], (D,), jnp.float32), 0.099609375, 1.8984375).astype(jnp.bfloat16),
        "w_recept": centred(streams_of[3], (D, WIDTH), D ** -0.5, 0.125, ((1, 2),)),
        "w_key": centred(streams_of[4], (D, WIDTH), D ** -0.5, 0.125, ((1, 2),)),
        "w_value": centred(streams_of[5], (D, WIDTH), D ** -0.5, 0.125, ((1, 2),)),
        "decay_down": centred(streams_of[6], (D, RANK), D ** -0.5, 0.125),
        "decay_up": centred(streams_of[7], (RANK, WIDTH), RANK ** -0.5, 0.75, ((1, 2),)),
        "decay_base": jnp.clip(-4.0 + 6.0 * jax.random.uniform(streams_of[8], (WIDTH,), jnp.float32) ** steps_of(streams_of[8], (WIDTH,), ((0, 2),), -0.2, 0.2), -4.0, 2.0),
        "iclr_down": centred(streams_of[9], (D, RANK), D ** -0.5, 0.125),
        "iclr_up": centred(streams_of[10], (RANK, WIDTH), RANK ** -0.5, 0.75, ((1, 2),)),
        "iclr_base": centred(streams_of[11], (WIDTH,), 1.0, 4.0, ((0, 2),), jnp.float32),
        "key_scale": jnp.clip(1.0 + 0.18 * jax.random.normal(streams_of[12], (WIDTH,), jnp.float32), 0.099609375, 1.8984375).astype(jnp.bfloat16),
        "key_mix": jnp.clip(1.0 + 0.18 * jax.random.normal(streams_of[13], (WIDTH,), jnp.float32), 0.099609375, 1.8984375).astype(jnp.bfloat16),
        "w_out": centred(streams_of[14], (WIDTH, D), (32 * WIDTH) ** -0.5, 0.046875, ((0, 2),)),
        "norm_moe": jnp.clip(1.0 + 0.18 * jax.random.normal(streams_of[15], (D,), jnp.float32), 0.099609375, 1.8984375).astype(jnp.bfloat16),
        "router_group": centred(streams_of[16], (D, GROUPS), D ** -0.5, 0.125),
        "router_expert": centred(streams_of[17], (D, EXPERTS), D ** -0.5, 0.125),
        "routes": draw_routes(jax.random.fold_in(streams_of[22], 71), 0),
        "expert_gate": centred(streams_of[19], (EXPERTS, D, FE), D ** -0.5, 0.125, ((0, 128), (2, 2))),
        "expert_up": centred(streams_of[20], (EXPERTS, D, FE), D ** -0.5, 0.125, ((0, 128), (2, 2))),
        "expert_down": centred(streams_of[21], (EXPERTS, FE, D), (FE // 16) ** -0.5, 1.5, ((0, 128), (1, 2))),
    }


def rms_scale(values, weights):
    values32 = values.astype(jnp.float32)
    factor = lax.rsqrt(lax.optimization_barrier(jnp.mean(values32 * values32, axis=-1, keepdims=True)) + 1e-06)
    return (values32 * factor * weights.astype(jnp.float32)).astype(jnp.bfloat16)

def split_heads(values):
    return values.astype(jnp.float32).reshape(values.shape[0], HEADS, HEAD)

def expert_rows(moe_rows, gate_weight, up_weight, down_weight):
    gate_part = jnp.dot(moe_rows, gate_weight, preferred_element_type=jnp.float32)
    up_part = jnp.dot(moe_rows, up_weight, preferred_element_type=jnp.float32)
    hidden = (jax.nn.silu(gate_part) * up_part).astype(jnp.bfloat16)
    block = FE // N_TP
    total = jnp.zeros((moe_rows.shape[0], D), jnp.float32)
    for index in range(N_TP):
        partial_value = jnp.dot(hidden[:, index * block:(index + 1) * block], down_weight[index * block:(index + 1) * block], preferred_element_type=jnp.float32).astype(jnp.bfloat16)
        partial_value = lax.optimization_barrier(partial_value)
        total = total + partial_value.astype(jnp.float32)
    return total.astype(jnp.bfloat16)

def reference(tokens_in, state_in, norm_mix, w_recept, w_key, w_value, decay_down, decay_up, decay_base, iclr_down, iclr_up, iclr_base, key_scale, key_mix, w_out, norm_moe, router_group, router_expert, routes, expert_gate, expert_up, expert_down):
    f32 = jnp.float32
    bf16 = jnp.bfloat16
    normed = rms_scale(tokens_in, norm_mix)
    recept = jnp.dot(normed, w_recept, preferred_element_type=f32).astype(bf16)
    key_rows = jnp.dot(normed, w_key, preferred_element_type=f32).astype(bf16)
    value_rows = jnp.dot(normed, w_value, preferred_element_type=f32).astype(bf16)
    decay_low = jnp.tanh(jnp.dot(normed, decay_down, preferred_element_type=f32)).astype(bf16)
    iclr_low = jnp.dot(normed, iclr_down, preferred_element_type=f32).astype(bf16)
    log_rate = -jax.nn.softplus(-(decay_base.astype(f32) + jnp.dot(decay_low, decay_up, preferred_element_type=f32))) - 0.5
    decays = jnp.exp(-jnp.exp(log_rate))
    learn_rate = jax.nn.sigmoid(iclr_base.astype(f32) + jnp.dot(iclr_low, iclr_up, preferred_element_type=f32))
    recept_heads = split_heads(recept)
    key_heads = split_heads(key_rows)
    value_heads = split_heads(value_rows)
    rate_heads = split_heads(learn_rate)
    decay_heads = split_heads(decays)
    scaled = key_heads * key_scale.astype(f32).reshape(HEADS, HEAD)
    unit_key = scaled * lax.rsqrt(lax.optimization_barrier(jnp.sum(scaled * scaled, axis=-1, keepdims=True)) + 1e-06)
    key_mod = key_heads * (1.0 + (rate_heads - 1.0) * key_mix.astype(f32).reshape(HEADS, HEAD))
    removed = jnp.einsum('shvk,shk->shv', state_in, unit_key)
    state_out = state_in * decay_heads[:, :, None, :] - removed[..., None] * (unit_key * rate_heads)[:, :, None, :] + value_heads[..., None] * key_mod[:, :, None, :]
    mixed = jnp.einsum('shvk,shk->shv', state_out, recept_heads).reshape(TOKENS, WIDTH).astype(bf16)
    mixer_out = jnp.dot(mixed, w_out, preferred_element_type=f32).astype(bf16)
    x_mid = (tokens_in.astype(f32) + mixer_out.astype(f32)).astype(bf16)
    moe_in = rms_scale(x_mid, norm_moe)
    group_id = routes[:, 0] // GROUP_EXPERTS
    group_logit = jnp.dot(moe_in, router_group, preferred_element_type=f32)
    group_hit = group_id[:, None] == jnp.arange(GROUPS, dtype=jnp.int32)[None, :]
    group_prob = jax.nn.sigmoid(lax.optimization_barrier(jnp.sum(jnp.where(group_hit, group_logit, 0.0), axis=1)))
    expert_logit = jnp.dot(moe_in, router_expert, preferred_element_type=f32)
    expert_hit = routes[:, :, None] == jnp.arange(EXPERTS, dtype=jnp.int32)[None, None, :]
    scores = jax.nn.sigmoid(lax.optimization_barrier(jnp.sum(jnp.where(expert_hit, expert_logit[:, None, :], 0.0), axis=2)))
    route_weight = group_prob[:, None] * scores / lax.optimization_barrier(jnp.sum(scores, axis=1, keepdims=True))
    limit = N_EP * CAP

    def visit(total, inputs):
        gate_weight, up_weight, down_weight, expert_index = inputs
        used = jnp.any(routes == expert_index, axis=1)
        found = jnp.nonzero(used, size=limit, fill_value=TOKENS)[0].astype(jnp.int32)
        valid = (found < TOKENS).astype(f32)
        safe = jnp.minimum(found, TOKENS - 1).astype(jnp.int32)
        results = expert_rows(moe_in[safe], gate_weight, up_weight, down_weight)
        weight = lax.optimization_barrier(jnp.sum(jnp.where(routes[safe] == expert_index, route_weight[safe], 0.0), axis=1)) * valid
        return (total.at[safe].add(weight[:, None] * results.astype(f32)), None)
    total, unused = lax.scan(visit, jnp.zeros((TOKENS, D), f32), (expert_gate, expert_up, expert_down, jnp.arange(EXPERTS, dtype=jnp.int32)))
    layer_out = (x_mid.astype(f32) + total).astype(bf16)
    return (layer_out, state_out)
```

```python
import jax
import jax.numpy as jnp
from jax import lax
from jax.experimental import pallas as pl
from jax.experimental.pallas import tpu as pltpu
from jax.sharding import PartitionSpec as P

MESH = pl.DeviceIdType.MESH
F32 = jnp.float32
BF16 = jnp.bfloat16
NZ, NY, NX = 8, 4, 4
NQ = NY * NX


def rms_scale(values, weights):
    values32 = values.astype(jnp.float32)
    factor = lax.rsqrt(jnp.mean(values32 * values32, axis=-1, keepdims=True) + 1e-06)
    return (values32 * factor * weights.astype(jnp.float32)).astype(jnp.bfloat16)


def iota(shape, dim):
    return lax.broadcasted_iota(jnp.int32, shape, dim)


def nt_dot(a, b):
    return lax.dot_general(a, b, (((1,), (1,)), ((), ())), preferred_element_type=F32)


def exchange_kernel(
    p1_ref, p1t_ref, meta_ref, src_ref, own_ref, gate_ref, up_ref, down_ref,
    out_ref,
    wg, wu, wd, send1, recv1, recvm, send2, recv2, part, partr, res, ret, comb, back,
    wsem, w_ss, w_rs, s1s, s1r, sms, smr, s2s, s2r, ps, pr, s3s, s3r, s4s, s4r,
):
    half = src_ref.shape[1]
    fh = gate_ref.shape[2]
    e = lax.axis_index("ep")
    t = lax.axis_index("tp")
    z, y, x = e // NQ, lax.rem(e // NX, NY), lax.rem(e, NX)
    me_q = lax.rem(e, NQ)
    partner = (e, 1 - t)

    def z_peer(d):
        return lax.rem(z + d + NZ, NZ) * NQ + me_q

    def q_of(a, b):
        return lax.rem(y + a + NY, NY) * NX + lax.rem(x + b + NX, NX)

    plane = [(a, b) for a in range(NY) for b in range(NX) if a or b]

    barrier = pltpu.get_barrier_semaphore()
    pl.semaphore_signal(barrier, inc=1, device_id=partner, device_id_type=MESH)
    for d in range(1, NZ):
        pl.semaphore_signal(barrier, inc=1, device_id=(z_peer(d), t), device_id_type=MESH)
    for a, b in plane:
        pl.semaphore_signal(barrier, inc=1, device_id=(z * NQ + q_of(a, b), t), device_id_type=MESH)

    mine = pl.ds(pl.multiple_of(t * half, half), half)
    theirs = pl.ds(pl.multiple_of((1 - t) * half, half), half)
    lanes = pl.ds(pl.multiple_of(t * fh, fh), fh)
    local = [
        pltpu.make_async_copy(gate_ref.at[0, mine], wg.at[:, lanes], wsem.at[0]),
        pltpu.make_async_copy(up_ref.at[0, mine], wu.at[:, lanes], wsem.at[1]),
        pltpu.make_async_copy(down_ref.at[0, :, mine], wd.at[lanes], wsem.at[2]),
    ]
    for copy in local:
        copy.start()

    rows = jnp.dot(p1_ref[...], src_ref[...], preferred_element_type=F32)
    for i in range(NZ):
        send1[i] = rows[8 * i : 8 * i + 8].astype(BF16)

    pl.semaphore_wait(barrier, NZ + NQ - 1)

    def remote(src, dst, ss, rs, device):
        copy = pltpu.make_async_remote_copy(src, dst, ss, rs, device_id=device, device_id_type=MESH)
        copy.start()
        return copy

    hop1 = []
    for d in range(1, NZ):
        zd = lax.rem(z + d, NZ)
        device = (z_peer(d), t)
        hop1.append(remote(meta_ref.at[zd], recvm.at[d], sms.at[d], smr.at[d], device))
        hop1.append(remote(send1.at[zd], recv1.at[d], s1s.at[d], s1r.at[d], device))
    weights = [
        remote(gate_ref.at[0, theirs], wg.at[:, lanes], w_ss.at[0], w_rs.at[0], partner),
        remote(up_ref.at[0, theirs], wu.at[:, lanes], w_ss.at[1], w_rs.at[1], partner),
        remote(down_ref.at[0, :, theirs], wd.at[lanes], w_ss.at[2], w_rs.at[2], partner),
    ]
    recv1[0] = send1[z]
    recvm[0] = meta_ref[z]

    col = iota((2 * NZ * NQ, 128), 0)
    chan = iota((2 * NZ * NQ, 128), 1)
    want = lax.rem(col, 2) * NQ + col // (2 * NZ)
    expand = jnp.where(chan == want, 1.0, 0.0).astype(BF16)
    expand_w = jnp.where(chan == want + 2 * NQ, 1.0, 0.0).astype(BF16)
    same_t = lax.rem(iota((2 * NZ * NQ, 64), 0) // 2, NZ) == iota((2 * NZ * NQ, 64), 1) // 8
    same = lax.rem(iota((64, 2 * NZ * NQ), 1) // 2, NZ) == iota((64, 2 * NZ * NQ), 0) // 8

    for copy in hop1:
        copy.wait_recv()
    meta = recvm[...].reshape(64, 128)
    meta_hi = meta.astype(BF16)
    choose = jnp.where(same_t, nt_dot(expand, meta_hi), 0.0).astype(BF16)
    arrived = recv1[...].astype(F32).reshape(64, half).astype(BF16)
    picked = jnp.dot(choose, arrived, preferred_element_type=F32).astype(BF16)
    send2[...] = picked.reshape(NQ, 2 * NZ, half)

    hop2 = []
    for i, (a, b) in enumerate(plane, 1):
        q = q_of(a, b)
        hop2.append(remote(send2.at[q], recv2.at[i], s2s.at[i], s2r.at[i], (z * NQ + q, t)))
    recv2[0] = send2[me_q]

    meta_lo = (meta - meta_hi.astype(F32)).astype(BF16)
    weigh_hi = jnp.where(same, nt_dot(meta_hi, expand_w), 0.0).astype(BF16)
    weigh_lo = jnp.where(same, nt_dot(meta_lo, expand_w), 0.0).astype(BF16)

    for copy in local:
        copy.wait()
    for copy in weights:
        copy.wait_recv()
    for copy in hop2:
        copy.wait_recv()

    flat = recv2[...].reshape(2 * NZ * NQ, half)
    gate_part = jnp.dot(flat, wg[...], preferred_element_type=F32)
    part[0] = gate_part.astype(BF16)
    gate_copy = remote(part.at[0], partr.at[0], ps.at[0], pr.at[0], partner)
    up_part = jnp.dot(flat, wu[...], preferred_element_type=F32)
    part[1] = up_part.astype(BF16)
    up_copy = remote(part.at[1], partr.at[1], ps.at[1], pr.at[1], partner)
    gate_copy.wait_recv()
    gate_sum = gate_part + partr[0].astype(F32)
    gated = gate_sum / (1.0 + jnp.exp(-gate_sum))
    up_copy.wait_recv()
    hidden = (gated * (up_part + partr[1].astype(F32))).astype(BF16)
    result = jnp.dot(hidden, wd[...], preferred_element_type=F32).astype(BF16)
    res[...] = result.reshape(NQ, 2 * NZ, half)

    hop3 = []
    for i, (a, b) in enumerate(plane, 1):
        q = q_of(-a, -b)
        hop3.append(remote(res.at[i], ret.at[me_q], s3s.at[i], s3r.at[i], (z * NQ + q, t)))
    ret[me_q] = res[0]
    for copy in hop3:
        copy.wait_recv()
    results = ret[...].reshape(2 * NZ * NQ, half)
    summed = jnp.dot(weigh_hi, results, preferred_element_type=F32)
    summed += jnp.dot(weigh_lo, results, preferred_element_type=F32)
    for i in range(NZ):
        comb[i] = summed[8 * i : 8 * i + 8].astype(BF16)

    hop4 = []
    for d in range(1, NZ):
        hop4.append(remote(comb.at[d], back.at[z], s4s.at[d], s4r.at[d], (z_peer(-d), t)))
    back[z] = comb[0]
    for copy in hop4:
        copy.wait_recv()
    sums = back[...].astype(F32).reshape(64, half).astype(BF16)
    moe_out = jnp.dot(p1t_ref[...], sums, preferred_element_type=F32)
    out_ref[...] = (own_ref[...].astype(F32) + moe_out).astype(BF16)

    for copy in hop1 + weights + hop2 + [gate_copy, up_copy] + hop3 + hop4:
        copy.wait_send()


def exchange(p1, p1t, meta, source, own_half, gate, up, down):
    rows, half = source.shape
    fh = gate.shape[2]
    slots = 2 * NZ * NQ
    vmem = pl.BlockSpec(memory_space=pltpu.VMEM)
    hbm = pl.BlockSpec(memory_space=pl.ANY)
    dma = pltpu.SemaphoreType.DMA
    return pl.pallas_call(
        exchange_kernel,
        out_shape=jax.ShapeDtypeStruct((rows, half), BF16),
        in_specs=[vmem] * 5 + [hbm] * 3,
        out_specs=vmem,
        scratch_shapes=[
            pltpu.VMEM((half, 2 * fh), BF16),
            pltpu.VMEM((half, 2 * fh), BF16),
            pltpu.VMEM((2 * fh, half), BF16),
            pltpu.VMEM((NZ, 8, half), BF16),
            pltpu.VMEM((NZ, 8, half), BF16),
            pltpu.VMEM((NZ, 8, 128), F32),
            pltpu.VMEM((NQ, 2 * NZ, half), BF16),
            pltpu.VMEM((NQ, 2 * NZ, half), BF16),
            pltpu.VMEM((2, slots, 2 * fh), BF16),
            pltpu.VMEM((2, slots, 2 * fh), BF16),
            pltpu.VMEM((NQ, 2 * NZ, half), BF16),
            pltpu.VMEM((NQ, 2 * NZ, half), BF16),
            pltpu.VMEM((NZ, 8, half), BF16),
            pltpu.VMEM((NZ, 8, half), BF16),
            dma((3,)), dma((3,)), dma((3,)),
            dma((NZ,)), dma((NZ,)), dma((NZ,)), dma((NZ,)),
            dma((NQ,)), dma((NQ,)),
            dma((2,)), dma((2,)),
            dma((NQ,)), dma((NQ,)),
            dma((NZ,)), dma((NZ,)),
        ],
        compiler_params=pltpu.CompilerParams(
            collective_id=0, has_side_effects=True, vmem_limit_bytes=32 * 1024 * 1024
        ),
    )(p1, p1t, meta, source, own_half, gate, up, down)


def total_of_pieces(value, axis):
    tiles = lax.all_gather(value, axis)
    return tiles.sum(axis=0)


def shards(
    tokens_in, state_in, norm_mix, w_recept, w_key, w_value, decay_down, decay_up, decay_base,
    iclr_down, iclr_up, iclr_base, key_scale, key_mix, w_out, norm_moe, router_group,
    router_expert, routes, expert_gate, expert_up, expert_down,
):
    f32 = jnp.float32
    bf16 = jnp.bfloat16
    seq_count = tokens_in.shape[0]
    width_model = tokens_in.shape[1]
    heads_here = state_in.shape[1]
    head_size = state_in.shape[-1]
    half_width = width_model // lax.axis_size("tp")

    def split_heads(values):
        return values.astype(f32).reshape(values.shape[0], heads_here, head_size)

    normed = rms_scale(tokens_in, norm_mix)
    recept = jnp.dot(normed, w_recept, preferred_element_type=f32).astype(bf16)
    key_rows = jnp.dot(normed, w_key, preferred_element_type=f32).astype(bf16)
    value_rows = jnp.dot(normed, w_value, preferred_element_type=f32).astype(bf16)
    decay_low = jnp.tanh(jnp.dot(normed, decay_down, preferred_element_type=f32)).astype(bf16)
    iclr_low = jnp.dot(normed, iclr_down, preferred_element_type=f32).astype(bf16)
    log_rate = (
        -jax.nn.softplus(-(decay_base + jnp.dot(decay_low, decay_up, preferred_element_type=f32)))
        - 0.5
    )
    decays = jnp.exp(-jnp.exp(log_rate))
    learn_rate = jax.nn.sigmoid(iclr_base + jnp.dot(iclr_low, iclr_up, preferred_element_type=f32))
    recept_heads = split_heads(recept)
    key_heads = split_heads(key_rows)
    value_heads = split_heads(value_rows)
    rate_heads = split_heads(learn_rate)
    decay_heads = split_heads(decays)
    scaled = key_heads * key_scale.astype(f32).reshape(heads_here, head_size)
    unit_key = scaled * lax.rsqrt(jnp.sum(scaled * scaled, axis=-1, keepdims=True) + 1e-06)
    key_mod = key_heads * (
        1.0 + (rate_heads - 1.0) * key_mix.astype(f32).reshape(heads_here, head_size)
    )
    removed = jnp.einsum("shvk,shk->shv", state_in, unit_key)
    state_out = (
        state_in * decay_heads[:, :, None, :]
        - removed[..., None] * (unit_key * rate_heads)[:, :, None, :]
        + value_heads[..., None] * key_mod[:, :, None, :]
    )
    mixed = (
        jnp.einsum("shvk,shk->shv", state_out, recept_heads)
        .reshape(seq_count, heads_here * head_size)
        .astype(bf16)
    )
    partial_value = jnp.dot(mixed, w_out, preferred_element_type=f32)
    mixer_out = total_of_pieces(partial_value, "tp").astype(bf16)
    x_mid = (tokens_in.astype(f32) + mixer_out.astype(f32)).astype(bf16)
    start = lax.axis_index("tp") * half_width
    own_half = lax.dynamic_slice_in_dim(x_mid, start, half_width, 1)
    moe_in = rms_scale(x_mid, norm_moe)
    n_groups = router_group.shape[1]
    experts_all = router_expert.shape[1]
    group_size = experts_all // n_groups
    group_id = routes[:, 0] // group_size
    group_logit = jnp.dot(moe_in, router_group, preferred_element_type=f32)
    group_hit = group_id[:, None] == jnp.arange(n_groups)[None, :]
    group_prob = jax.nn.sigmoid(jnp.sum(jnp.where(group_hit, group_logit, 0.0), axis=1))
    expert_logit = jnp.dot(moe_in, router_expert, preferred_element_type=f32)
    expert_hit = routes[:, :, None] == jnp.arange(experts_all)[None, None, :]
    scores = jax.nn.sigmoid(jnp.sum(jnp.where(expert_hit, expert_logit[:, None, :], 0.0), axis=2))
    route_weight = group_prob[:, None] * scores / jnp.sum(scores, axis=1, keepdims=True)

    order = jnp.arange(seq_count)
    named_before = jnp.sum(
        (routes[:, :, None, None] == routes[None, None, :, :]) & (order[:, None] > order)[:, None, :, None],
        axis=(2, 3),
    )
    rank = jnp.sum((group_id[:, None] == group_id[None, :]) & (order[:, None] > order[None, :]), axis=1)
    slot = group_id * 4 + rank
    p1t = slot[:, None] == jnp.arange(64)[None, :]
    channel = named_before * NQ + routes % NQ
    chans = jnp.arange(128)[None, None, :]
    tok_meta = jnp.sum(
        jnp.where(channel[:, :, None] == chans, 1.0, 0.0)
        + jnp.where(channel[:, :, None] + 2 * NQ == chans, route_weight[:, :, None], 0.0),
        axis=1,
    )
    p1 = p1t.T
    meta = jnp.dot(p1.astype(f32), tok_meta, precision=lax.Precision.HIGHEST).reshape(NZ, 8, 128)
    source = lax.dynamic_slice_in_dim(moe_in, start, half_width, 1)
    layer_out = exchange(
        p1.astype(bf16), p1t.astype(bf16), meta, source, own_half, expert_gate, expert_up, expert_down
    )
    return (layer_out, state_out)


def solution(mesh):
    in_specs = (
        P("ep", None),
        P("ep", "tp", None, None),
        P(),
        P(None, "tp"),
        P(None, "tp"),
        P(None, "tp"),
        P(),
        P(None, "tp"),
        P("tp"),
        P(),
        P(None, "tp"),
        P("tp"),
        P("tp"),
        P("tp"),
        P("tp", None),
        P(),
        P(),
        P(),
        P("ep", None),
        P("ep", None, "tp"),
        P("ep", None, "tp"),
        P("ep", "tp", None),
    )
    out_specs = (P("ep", "tp"), P("ep", "tp", None, None))
    return jax.shard_map(shards, mesh=mesh, in_specs=in_specs, out_specs=out_specs, check_vma=False)
```

```python
import math

import jax
import jax.numpy as jnp
from jax import lax
from jax.experimental import pallas as pl
from jax.experimental.pallas import tpu as pltpu
from jax.sharding import PartitionSpec as P

MESH = pl.DeviceIdType.MESH
F32 = jnp.float32
BF16 = jnp.bfloat16
NZ, NY, NX = 8, 4, 4
NQ = NY * NX


def iota(shape, dim):
    return lax.broadcasted_iota(jnp.int32, shape, dim)


def one_hot(where):
    return jnp.where(where, 1.0, 0.0).astype(BF16)


def nt_dot(a, b):
    return lax.dot_general(a, b, (((1,), (1,)), ((), ())), preferred_element_type=F32)


def scale_rows(values32, gain):
    mean = jnp.mean(values32 * values32, axis=-1, keepdims=True)
    return (values32 * lax.rsqrt(mean + 1e-06) * gain).astype(BF16)


def sigmoid(u):
    return 1.0 / (1.0 + jnp.exp(-u))


def split_dot(a, b):
    hi = a.astype(BF16)
    lo = (a - hi.astype(F32)).astype(BF16)
    return jnp.dot(hi, b, preferred_element_type=F32) + jnp.dot(lo, b, preferred_element_type=F32)


def front_kernel(
    tok_ref, norm_ref, wr_ref, wk_ref, wv_ref, dd_ref, du_ref, db_ref, id_ref, iu_ref, ib_ref,
    ks_ref, km_ref, wo_ref, state_ref,
    partial_ref, state_out_ref,
    tok, norm, wr, wk, wv, dd, du, db, idn, iu, ib, ks, km, wo, sin, sout, lhs, decay, tall,
    isem, ssem, osem,
):
    seqs, heads, hs, _ = state_ref.shape
    width = heads * hs
    chunk = 8
    chunks = seqs // chunk
    loads = {}
    order = [
        ("tok", tok_ref, tok), ("norm", norm_ref, norm), ("wk", wk_ref, wk), ("dd", dd_ref, dd), ("id", id_ref, idn),
        ("wv", wv_ref, wv), ("wr", wr_ref, wr), ("du", du_ref, du), ("db", db_ref, db), ("iu", iu_ref, iu),
        ("ib", ib_ref, ib), ("ks", ks_ref, ks), ("km", km_ref, km),
    ]
    for i, (name, src, dst) in enumerate(order):
        loads[name] = pltpu.make_async_copy(src, dst, isem.at[i])
        loads[name].start()
    states = []
    for c in range(chunks):
        rows = pl.ds(c * chunk, chunk)
        states.append(pltpu.make_async_copy(state_ref.at[rows], sin.at[rows], ssem.at[c]))
        states[c].start()
    loads["wo"] = pltpu.make_async_copy(wo_ref, wo, isem.at[len(order)])
    loads["wo"].start()

    def got(*names):
        for name in names:
            loads[name].wait()

    got("tok", "norm")
    normed = scale_rows(tok[...].astype(F32), norm[...].astype(F32).reshape(1, -1))

    def project(weight):
        return jnp.dot(normed, weight[...], preferred_element_type=F32).astype(BF16)

    got("wk")
    key = project(wk).astype(F32)
    got("dd", "id")
    decay_low = jnp.tanh(nt_dot(normed, dd[...])).astype(BF16)
    iclr_low = nt_dot(normed, idn[...]).astype(BF16)
    got("wv", "wr")
    value = project(wv)
    recept = project(wr)
    got("du", "db", "iu", "ib", "ks", "km")
    rate_in = db[...].reshape(1, -1) + jnp.dot(decay_low, du[...], preferred_element_type=F32)
    decays = jnp.exp(-math.exp(-0.5) * sigmoid(rate_in))
    learn = sigmoid(ib[...].reshape(1, -1) + jnp.dot(iclr_low, iu[...], preferred_element_type=F32))
    scaled = key * ks[...].astype(F32).reshape(1, -1)
    head_ones = jnp.where(iota((width, width), 0) // hs == iota((width, width), 1) // hs, 1.0, 0.0).astype(BF16)
    unit_key = scaled * lax.rsqrt(split_dot(scaled * scaled, head_ones) + 1e-06)
    key_mod = key * (1.0 + (learn - 1.0) * km[...].astype(F32).reshape(1, -1))

    def by_head(values):
        return jnp.concatenate([values[:, h * hs : (h + 1) * hs] for h in range(heads)], axis=0)

    pairs = heads * seqs
    decay[...] = by_head(decays)
    keys_u = by_head(unit_key).astype(BF16)
    right = jnp.concatenate([by_head(-unit_key * learn), by_head(key_mod)], axis=0).astype(BF16)
    reads = by_head(recept.astype(F32)).astype(BF16)
    pick = jnp.where(iota((seqs, pairs), 0) == lax.rem(iota((seqs, pairs), 1), seqs), 1.0, 0.0).astype(BF16)
    spread = lax.dot_general(value, pick, (((0,), (0,)), ((), ())), preferred_element_type=F32)

    lane = iota((hs, pairs), 1)
    tall[...] = jnp.zeros_like(tall)
    for c in range(chunks):
        states[c].wait()
        for s in range(c * chunk, (c + 1) * chunk):
            found = nt_dot(sin[s].reshape(width, hs).astype(BF16), keys_u)
            for h in range(heads):
                own = lane == h * seqs + s
                rows = slice(h * hs, (h + 1) * hs)
                lhs[s - c * chunk, rows, :pairs] = jnp.where(own, found[rows], 0.0).astype(BF16)
                lhs[s - c * chunk, rows, pairs:] = jnp.where(own, spread[rows], 0.0).astype(BF16)
        for s in range(c * chunk, (c + 1) * chunk):
            update = jnp.dot(lhs[s - c * chunk], right, preferred_element_type=F32)
            for h in range(heads):
                row = h * seqs + s
                sout[s, h] = sin[s, h] * decay[row : row + 1, :] + update[h * hs : (h + 1) * hs]
        rows = pl.ds(c * chunk, chunk)
        pltpu.make_async_copy(sout.at[rows], state_out_ref.at[rows], osem.at[c]).start()
        for s in range(c * chunk, (c + 1) * chunk):
            seen = nt_dot(sout[s].reshape(width, hs).astype(BF16), reads)
            for h in range(heads):
                rows = slice(h * hs, (h + 1) * hs)
                tall[rows] = jnp.where(lane == h * seqs + s, seen[rows], tall[rows])
    mixed = nt_dot(pick, tall[...].astype(BF16)).astype(BF16)
    got("wo")
    partial_ref[...] = jnp.dot(mixed, wo[...], preferred_element_type=F32)
    for c in range(chunks):
        rows = pl.ds(c * chunk, chunk)
        pltpu.make_async_copy(sout.at[rows], state_out_ref.at[rows], osem.at[c]).wait()


def front(tok, norm, wr, wk, wv, dd, du, db, idn, iu, ib, ks, km, wo, state):
    seqs, heads, hs, _ = state.shape
    width, pairs = heads * hs, heads * seqs
    hbm = pl.BlockSpec(memory_space=pltpu.HBM)
    args = (tok, norm, wr, wk, wv, dd, du, db, idn, iu, ib, ks, km, wo)
    return pl.pallas_call(
        front_kernel,
        out_shape=(
            jax.ShapeDtypeStruct(tok.shape, F32),
            jax.ShapeDtypeStruct(state.shape, F32),
        ),
        in_specs=[hbm] * 15,
        out_specs=(pl.BlockSpec(memory_space=pltpu.VMEM), hbm),
        scratch_shapes=[pltpu.VMEM(a.shape, a.dtype) for a in args]
        + [
            pltpu.VMEM(state.shape, F32),
            pltpu.VMEM(state.shape, F32),
            pltpu.VMEM((8, width, 2 * pairs), BF16),
            pltpu.VMEM((pairs, hs), F32),
            pltpu.VMEM((width, pairs), F32),
            pltpu.SemaphoreType.DMA((len(args),)),
            pltpu.SemaphoreType.DMA((seqs // 8,)),
            pltpu.SemaphoreType.DMA((seqs // 8,)),
        ],
        compiler_params=pltpu.CompilerParams(vmem_limit_bytes=67043328),
    )(*args, state)


def exchange_kernel(
    pieces_ref, tok_ref, norm_ref, rg_ref, re_ref, routes_ref, gate_ref, up_ref, down_ref,
    out_ref,
    pieces, tok, norm, rg, rex, routes, xm, moe,
    wg, wu, wd, sendc, recvc, send1, recv1, sendm, recvm, send2, recv2, part, partr, res, ret, comb, back,
    isem, wsem, w_ss, w_rs, scs, scr, s1s, s1r, sms, smr, s2s, s2r, ps, pr, s3s, s3r, s4s, s4r,
):
    seqs, half = out_ref.shape
    fh = gate_ref.shape[2]
    experts = re_ref.shape[1]
    groups = rg_ref.shape[0]
    e = lax.axis_index("ep")
    t = lax.axis_index("tp")
    z, y, x = e // NQ, lax.rem(e // NX, NY), lax.rem(e, NX)
    me_q = lax.rem(e, NQ)
    partner = (e, 1 - t)

    def z_peer(d):
        return lax.rem(z + d + NZ, NZ) * NQ + me_q

    def q_of(a, b):
        return lax.rem(y + a + NY, NY) * NX + lax.rem(x + b + NX, NX)

    plane = [(a, b) for a in range(NY) for b in range(NX) if a or b]

    barrier = pltpu.get_barrier_semaphore()
    pl.semaphore_signal(barrier, inc=1, device_id=partner, device_id_type=MESH)
    for d in range(1, NZ):
        pl.semaphore_signal(barrier, inc=1, device_id=(z_peer(d), t), device_id_type=MESH)
    for a, b in plane:
        pl.semaphore_signal(barrier, inc=1, device_id=(z * NQ + q_of(a, b), t), device_id_type=MESH)

    mine = pl.ds(pl.multiple_of(t * half, half), half)
    theirs = pl.ds(pl.multiple_of((1 - t) * half, half), half)
    lanes = pl.ds(pl.multiple_of(t * fh, fh), fh)
    local = [
        pltpu.make_async_copy(gate_ref.at[0, mine], wg.at[:, lanes], wsem.at[0]),
        pltpu.make_async_copy(up_ref.at[0, mine], wu.at[:, lanes], wsem.at[1]),
        pltpu.make_async_copy(down_ref.at[0, :, mine], wd.at[lanes], wsem.at[2]),
    ]
    loads = {}
    for i, (name, src, dst) in enumerate([
        ("routes", routes_ref, routes), ("pieces", pieces_ref, pieces), ("tok", tok_ref, tok), ("norm", norm_ref, norm),
        ("rex", re_ref, rex), ("rg", rg_ref, rg),
    ]):
        loads[name] = pltpu.make_async_copy(src, dst, isem.at[i])
        loads[name].start()
    for copy in local:
        copy.start()

    loads["routes"].wait()
    table = jnp.concatenate([routes[...].astype(F32), jnp.zeros_like(routes, F32)], axis=0).astype(BF16)
    named = nt_dot(one_hot(iota((seqs, seqs), 0) == iota((seqs, seqs), 1)), table)
    expert_lane = iota((seqs, experts), 1).astype(F32)
    hit = jnp.zeros((seqs, experts), F32)
    for k in range(routes.shape[0]):
        hit += jnp.where(named[:, k : k + 1] == expert_lane, 1.0, 0.0)
    earlier = one_hot(iota((seqs, seqs), 1) < iota((seqs, seqs), 0))
    first = jnp.where(jnp.dot(earlier, hit.astype(BF16), preferred_element_type=F32) < 0.5, hit, 0.0)
    fold_row = iota((2 * experts, 128), 0)
    fold = one_hot(iota((2 * experts, 128), 1) == (fold_row // experts) * NQ + lax.rem(fold_row, NQ))
    group_of = one_hot(iota((experts, groups), 0) // (experts // groups) == iota((experts, groups), 1))
    in_group = jnp.where(jnp.dot(hit.astype(BF16), group_of, preferred_element_type=F32) > 0.5, 1.0, 0.0)
    before = jnp.dot(earlier, in_group.astype(BF16), preferred_element_type=F32)
    slot = jnp.sum(in_group * (4.0 * iota((seqs, groups), 1).astype(F32) + before), axis=1, keepdims=True)
    p1t = one_hot(slot == iota((seqs, 64), 1).astype(F32))
    p1 = nt_dot(one_hot(iota((64, 64), 0) == iota((64, 64), 1)), p1t).astype(BF16)
    ranked = jnp.concatenate([first, hit - first], axis=1)
    choice = jnp.dot(ranked.astype(BF16), fold, preferred_element_type=F32).astype(BF16)
    choice = jnp.dot(p1, choice, preferred_element_type=F32)
    for i in range(NZ):
        sendc[i] = choice[8 * i : 8 * i + 8].astype(BF16)

    for name in ("pieces", "tok", "norm"):
        loads[name].wait()
    mixer_out = (pieces[0] + pieces[1]).astype(BF16)
    x_mid = (tok[...].astype(F32) + mixer_out.astype(F32)).astype(BF16)
    moe_in = scale_rows(x_mid.astype(F32), norm[...].astype(F32).reshape(1, -1))
    for i in range(2):
        xm[i] = x_mid[:, i * half : (i + 1) * half]
        moe[i] = moe_in[:, i * half : (i + 1) * half]
    rows = jnp.dot(p1, moe[t], preferred_element_type=F32)
    for i in range(NZ):
        send1[i] = rows[8 * i : 8 * i + 8].astype(BF16)

    pl.semaphore_wait(barrier, NZ + NQ - 1)

    def remote(src, dst, ss, rs, device):
        copy = pltpu.make_async_remote_copy(src, dst, ss, rs, device_id=device, device_id_type=MESH)
        copy.start()
        return copy

    hop1 = []
    for d in range(1, NZ):
        zd = lax.rem(z + d, NZ)
        hop1.append(remote(sendc.at[zd], recvc.at[d], scs.at[d], scr.at[d], (z_peer(d), t)))
        hop1.append(remote(send1.at[zd], recv1.at[d], s1s.at[d], s1r.at[d], (z_peer(d), t)))
    weights = [
        remote(gate_ref.at[0, theirs], wg.at[:, lanes], w_ss.at[0], w_rs.at[0], partner),
        remote(up_ref.at[0, theirs], wu.at[:, lanes], w_ss.at[1], w_rs.at[1], partner),
        remote(down_ref.at[0, :, theirs], wd.at[lanes], w_ss.at[2], w_rs.at[2], partner),
    ]
    recvc[0] = sendc[z]
    recv1[0] = send1[z]

    loads["rex"].wait()
    loads["rg"].wait()
    scores = hit * sigmoid(jnp.dot(moe_in, rex[...], preferred_element_type=F32))
    group_prob = sigmoid(jnp.sum(in_group * nt_dot(moe_in, rg[...]), axis=1, keepdims=True))
    route_weight = group_prob * scores / jnp.sum(scores, axis=1, keepdims=True)
    weighed = jnp.concatenate([route_weight * first, route_weight * (hit - first)], axis=1)
    weighed = split_dot(weighed, fold)
    high = weighed.astype(BF16)
    low = (weighed - high.astype(F32)).astype(BF16)
    sendm[...] = (
        jnp.dot(p1, high, preferred_element_type=F32) + jnp.dot(p1, low, preferred_element_type=F32)
    ).reshape(NZ, 8, 128)
    hopw = []
    for d in range(1, NZ):
        zd = lax.rem(z + d, NZ)
        hopw.append(remote(sendm.at[zd], recvm.at[d], sms.at[d], smr.at[d], (z_peer(d), t)))
    recvm[0] = sendm[z]

    col = iota((2 * NZ * NQ, 128), 0)
    chan = iota((2 * NZ * NQ, 128), 1)
    want = lax.rem(col, 2) * NQ + col // (2 * NZ)
    expand = one_hot(chan == want)
    same_t = lax.rem(iota((2 * NZ * NQ, 64), 0) // 2, NZ) == iota((2 * NZ * NQ, 64), 1) // 8
    same = lax.rem(iota((64, 2 * NZ * NQ), 1) // 2, NZ) == iota((64, 2 * NZ * NQ), 0) // 8

    for copy in hop1:
        copy.wait_recv()
    chosen = recvc[...].astype(F32).reshape(64, 128).astype(BF16)
    choose = jnp.where(same_t, nt_dot(expand, chosen), 0.0).astype(BF16)
    arrived = recv1[...].astype(F32).reshape(64, half).astype(BF16)
    picked = jnp.dot(choose, arrived, preferred_element_type=F32).astype(BF16)
    send2[...] = picked.reshape(NQ, 2 * NZ, half)

    hop2 = []
    for i, (a, b) in enumerate(plane, 1):
        q = q_of(a, b)
        hop2.append(remote(send2.at[q], recv2.at[i], s2s.at[i], s2r.at[i], (z * NQ + q, t)))
    recv2[0] = send2[me_q]

    for copy in hopw:
        copy.wait_recv()
    meta = recvm[...].reshape(64, 128)
    meta_hi = meta.astype(BF16)
    meta_lo = (meta - meta_hi.astype(F32)).astype(BF16)
    weigh_hi = jnp.where(same, nt_dot(meta_hi, expand), 0.0).astype(BF16)
    weigh_lo = jnp.where(same, nt_dot(meta_lo, expand), 0.0).astype(BF16)

    for copy in local:
        copy.wait()
    for copy in weights:
        copy.wait_recv()
    for copy in hop2:
        copy.wait_recv()

    flat = recv2[...].reshape(2 * NZ * NQ, half)
    gate_part = jnp.dot(flat, wg[...], preferred_element_type=F32)
    part[0] = gate_part.astype(BF16)
    gate_copy = remote(part.at[0], partr.at[0], ps.at[0], pr.at[0], partner)
    up_part = jnp.dot(flat, wu[...], preferred_element_type=F32)
    part[1] = up_part.astype(BF16)
    up_copy = remote(part.at[1], partr.at[1], ps.at[1], pr.at[1], partner)
    gate_copy.wait_recv()
    gate_sum = gate_part + partr[0].astype(F32)
    gated = gate_sum / (1.0 + jnp.exp(-gate_sum))
    up_copy.wait_recv()
    hidden = (gated * (up_part + partr[1].astype(F32))).astype(BF16)
    result = jnp.dot(hidden, wd[...], preferred_element_type=F32).astype(BF16)
    res[...] = result.reshape(NQ, 2 * NZ, half)

    hop3 = []
    for i, (a, b) in enumerate(plane, 1):
        q = q_of(-a, -b)
        hop3.append(remote(res.at[i], ret.at[me_q], s3s.at[i], s3r.at[i], (z * NQ + q, t)))
    ret[me_q] = res[0]
    for copy in hop3:
        copy.wait_recv()
    results = ret[...].reshape(2 * NZ * NQ, half)
    summed = jnp.dot(weigh_hi, results, preferred_element_type=F32)
    summed += jnp.dot(weigh_lo, results, preferred_element_type=F32)
    for i in range(NZ):
        comb[i] = summed[8 * i : 8 * i + 8].astype(BF16)

    hop4 = []
    for d in range(1, NZ):
        hop4.append(remote(comb.at[d], back.at[z], s4s.at[d], s4r.at[d], (z_peer(-d), t)))
    back[z] = comb[0]
    for copy in hop4:
        copy.wait_recv()
    sums = back[...].astype(F32).reshape(64, half).astype(BF16)
    moe_out = jnp.dot(p1t, sums, preferred_element_type=F32)
    out_ref[...] = (xm[t].astype(F32) + moe_out).astype(BF16)

    for copy in hop1 + hopw + weights + hop2 + [gate_copy, up_copy] + hop3 + hop4:
        copy.wait_send()


def exchange(pieces, tok, norm, rg, rex, routes, gate, up, down):
    seqs, half = tok.shape[0], tok.shape[1] // 2
    fh = gate.shape[2]
    slots = 2 * NZ * NQ
    vmem = pl.BlockSpec(memory_space=pltpu.VMEM)
    hbm = pl.BlockSpec(memory_space=pl.ANY)
    dma = pltpu.SemaphoreType.DMA
    small = (pieces, tok, norm, rg, rex, routes)
    by_z = pltpu.VMEM((NZ, 8, half), BF16)
    by_q = pltpu.VMEM((NQ, 2 * NZ, half), BF16)
    return pl.pallas_call(
        exchange_kernel,
        out_shape=jax.ShapeDtypeStruct((seqs, half), BF16),
        in_specs=[hbm] * 9,
        out_specs=vmem,
        scratch_shapes=[pltpu.VMEM(a.shape, a.dtype) for a in small]
        + [
            pltpu.VMEM((2, seqs, half), BF16),
            pltpu.VMEM((2, seqs, half), BF16),
            pltpu.VMEM((half, 2 * fh), BF16),
            pltpu.VMEM((half, 2 * fh), BF16),
            pltpu.VMEM((2 * fh, half), BF16),
            pltpu.VMEM((NZ, 8, 128), BF16),
            pltpu.VMEM((NZ, 8, 128), BF16),
            by_z,
            by_z,
            pltpu.VMEM((NZ, 8, 128), F32),
            pltpu.VMEM((NZ, 8, 128), F32),
            by_q,
            by_q,
            pltpu.VMEM((2, slots, 2 * fh), BF16),
            pltpu.VMEM((2, slots, 2 * fh), BF16),
            by_q,
            by_q,
            by_z,
            by_z,
            dma((len(small),)),
            dma((3,)), dma((3,)), dma((3,)),
            dma((NZ,)), dma((NZ,)), dma((NZ,)), dma((NZ,)), dma((NZ,)), dma((NZ,)),
            dma((NQ,)), dma((NQ,)),
            dma((2,)), dma((2,)),
            dma((NQ,)), dma((NQ,)),
            dma((NZ,)), dma((NZ,)),
        ],
        compiler_params=pltpu.CompilerParams(
            collective_id=0, has_side_effects=True, vmem_limit_bytes=67043328
        ),
    )(*small, gate, up, down)


def shards(
    tokens_in, state_in, norm_mix, w_recept, w_key, w_value, decay_down, decay_up, decay_base,
    iclr_down, iclr_up, iclr_base, key_scale, key_mix, w_out, norm_moe, router_group,
    router_expert, routes, expert_gate, expert_up, expert_down,
):
    partial_value, state_out = front(
        tokens_in, norm_mix, w_recept, w_key, w_value, decay_down.T, decay_up, decay_base,
        iclr_down.T, iclr_up, iclr_base, key_scale, key_mix, w_out, state_in,
    )
    layer_out = exchange(
        lax.all_gather(partial_value, "tp"), tokens_in, norm_moe, router_group.T, router_expert, routes.T,
        expert_gate, expert_up, expert_down,
    )
    return (layer_out, state_out)


def solution(mesh):
    in_specs = (
        P("ep", None),
        P("ep", "tp", None, None),
        P(),
        P(None, "tp"),
        P(None, "tp"),
        P(None, "tp"),
        P(),
        P(None, "tp"),
        P("tp"),
        P(),
        P(None, "tp"),
        P("tp"),
        P("tp"),
        P("tp"),
        P("tp", None),
        P(),
        P(),
        P(),
        P("ep", None),
        P("ep", None, "tp"),
        P("ep", None, "tp"),
        P("ep", "tp", None),
    )
    out_specs = (P("ep", "tp"), P("ep", "tp", None, None))
    return jax.shard_map(shards, mesh=mesh, in_specs=in_specs, out_specs=out_specs, check_vma=False)
```

```python
import math

import jax
import jax.numpy as jnp
from jax import lax
from jax.experimental import pallas as pl
from jax.experimental.pallas import tpu as pltpu
from jax.sharding import PartitionSpec as P

MESH = pl.DeviceIdType.MESH
F32 = jnp.float32
BF16 = jnp.bfloat16
NZ, NY, NX = 8, 4, 4
NQ = NY * NX
ORDER = (0, 1, 7, 2, 6, 3, 5, 4)
BATCH = NZ // 2


def iota(shape, dim):
    return lax.broadcasted_iota(jnp.int32, shape, dim)


def one_hot(where):
    return jnp.where(where, 1.0, 0.0).astype(BF16)


def nt_dot(a, b):
    return lax.dot_general(a, b, (((1,), (1,)), ((), ())), preferred_element_type=F32)


def scale_rows(values32, gain):
    mean = jnp.mean(values32 * values32, axis=-1, keepdims=True)
    return (values32 * lax.rsqrt(mean + 1e-06) * gain).astype(BF16)


def sigmoid(u):
    return 1.0 / (1.0 + jnp.exp(-u))


def split_dot(a, b):
    hi = a.astype(BF16)
    lo = (a - hi.astype(F32)).astype(BF16)
    return jnp.dot(hi, b, preferred_element_type=F32) + jnp.dot(lo, b, preferred_element_type=F32)


def front_kernel(
    tok_ref, norm_ref, wr_ref, wk_ref, wv_ref, dd_ref, du_ref, db_ref, id_ref, iu_ref, ib_ref,
    ks_ref, km_ref, wo_ref, state_ref,
    partial_ref, state_out_ref,
    tok, norm, wr, wk, wv, dd, du, db, idn, iu, ib, ks, km, wo, sin, sout, lhs, decay, tall,
    isem, ssem, osem,
):
    seqs, heads, hs, _ = state_ref.shape
    width = heads * hs
    chunk = 8
    chunks = seqs // chunk
    loads = {}
    order = [
        ("tok", tok_ref, tok), ("norm", norm_ref, norm), ("wk", wk_ref, wk), ("dd", dd_ref, dd), ("id", id_ref, idn),
        ("wv", wv_ref, wv), ("wr", wr_ref, wr), ("du", du_ref, du), ("db", db_ref, db), ("iu", iu_ref, iu),
        ("ib", ib_ref, ib), ("ks", ks_ref, ks), ("km", km_ref, km),
    ]
    for i, (name, src, dst) in enumerate(order):
        loads[name] = pltpu.make_async_copy(src, dst, isem.at[i])
        loads[name].start()
    states = []
    for c in range(chunks):
        rows = pl.ds(c * chunk, chunk)
        states.append(pltpu.make_async_copy(state_ref.at[rows], sin.at[rows], ssem.at[c]))
        states[c].start()
    loads["wo"] = pltpu.make_async_copy(wo_ref, wo, isem.at[len(order)])
    loads["wo"].start()

    def got(*names):
        for name in names:
            loads[name].wait()

    got("tok", "norm")
    normed = scale_rows(tok[...].astype(F32), norm[...].astype(F32).reshape(1, -1))

    def project(weight):
        return jnp.dot(normed, weight[...], preferred_element_type=F32).astype(BF16)

    got("wk")
    key = project(wk).astype(F32)
    got("dd", "id")
    decay_low = jnp.tanh(nt_dot(normed, dd[...])).astype(BF16)
    iclr_low = nt_dot(normed, idn[...]).astype(BF16)
    got("wv", "wr")
    value = project(wv)
    recept = project(wr)
    got("du", "db", "iu", "ib", "ks", "km")
    rate_in = db[...].reshape(1, -1) + jnp.dot(decay_low, du[...], preferred_element_type=F32)
    decays = jnp.exp(-math.exp(-0.5) * sigmoid(rate_in))
    learn = sigmoid(ib[...].reshape(1, -1) + jnp.dot(iclr_low, iu[...], preferred_element_type=F32))
    scaled = key * ks[...].astype(F32).reshape(1, -1)
    head_ones = jnp.where(iota((width, width), 0) // hs == iota((width, width), 1) // hs, 1.0, 0.0).astype(BF16)
    unit_key = scaled * lax.rsqrt(split_dot(scaled * scaled, head_ones) + 1e-06)
    key_mod = key * (1.0 + (learn - 1.0) * km[...].astype(F32).reshape(1, -1))

    def by_head(values):
        return jnp.concatenate([values[:, h * hs : (h + 1) * hs] for h in range(heads)], axis=0)

    pairs = heads * seqs
    decay[...] = by_head(decays)
    keys_u = by_head(unit_key).astype(BF16)
    right = jnp.concatenate([by_head(-unit_key * learn), by_head(key_mod)], axis=0).astype(BF16)
    reads = by_head(recept.astype(F32)).astype(BF16)
    pick = jnp.where(iota((seqs, pairs), 0) == lax.rem(iota((seqs, pairs), 1), seqs), 1.0, 0.0).astype(BF16)
    spread = lax.dot_general(value, pick, (((0,), (0,)), ((), ())), preferred_element_type=F32)

    lane = iota((hs, pairs), 1)
    tall[...] = jnp.zeros_like(tall)
    for c in range(chunks):
        states[c].wait()
        for s in range(c * chunk, (c + 1) * chunk):
            found = nt_dot(sin[s].reshape(width, hs).astype(BF16), keys_u)
            for h in range(heads):
                own = lane == h * seqs + s
                rows = slice(h * hs, (h + 1) * hs)
                lhs[s - c * chunk, rows, :pairs] = jnp.where(own, found[rows], 0.0).astype(BF16)
                lhs[s - c * chunk, rows, pairs:] = jnp.where(own, spread[rows], 0.0).astype(BF16)
        for s in range(c * chunk, (c + 1) * chunk):
            update = jnp.dot(lhs[s - c * chunk], right, preferred_element_type=F32)
            for h in range(heads):
                row = h * seqs + s
                sout[s, h] = sin[s, h] * decay[row : row + 1, :] + update[h * hs : (h + 1) * hs]
        rows = pl.ds(c * chunk, chunk)
        pltpu.make_async_copy(sout.at[rows], state_out_ref.at[rows], osem.at[c]).start()
        for s in range(c * chunk, (c + 1) * chunk):
            seen = nt_dot(sout[s].reshape(width, hs).astype(BF16), reads)
            for h in range(heads):
                rows = slice(h * hs, (h + 1) * hs)
                tall[rows] = jnp.where(lane == h * seqs + s, seen[rows], tall[rows])
    mixed = nt_dot(pick, tall[...].astype(BF16)).astype(BF16)
    got("wo")
    partial_ref[...] = jnp.dot(mixed, wo[...], preferred_element_type=F32)
    for c in range(chunks):
        rows = pl.ds(c * chunk, chunk)
        pltpu.make_async_copy(sout.at[rows], state_out_ref.at[rows], osem.at[c]).wait()


def front(tok, norm, wr, wk, wv, dd, du, db, idn, iu, ib, ks, km, wo, state):
    seqs, heads, hs, _ = state.shape
    width, pairs = heads * hs, heads * seqs
    hbm = pl.BlockSpec(memory_space=pltpu.HBM)
    args = (tok, norm, wr, wk, wv, dd, du, db, idn, iu, ib, ks, km, wo)
    return pl.pallas_call(
        front_kernel,
        out_shape=(
            jax.ShapeDtypeStruct(tok.shape, F32),
            jax.ShapeDtypeStruct(state.shape, F32),
        ),
        in_specs=[hbm] * 15,
        out_specs=(pl.BlockSpec(memory_space=pltpu.VMEM), hbm),
        scratch_shapes=[pltpu.VMEM(a.shape, a.dtype) for a in args]
        + [
            pltpu.VMEM(state.shape, F32),
            pltpu.VMEM(state.shape, F32),
            pltpu.VMEM((8, width, 2 * pairs), BF16),
            pltpu.VMEM((pairs, hs), F32),
            pltpu.VMEM((width, pairs), F32),
            pltpu.SemaphoreType.DMA((len(args),)),
            pltpu.SemaphoreType.DMA((seqs // 8,)),
            pltpu.SemaphoreType.DMA((seqs // 8,)),
        ],
        compiler_params=pltpu.CompilerParams(vmem_limit_bytes=67043328),
    )(*args, state)


def exchange_kernel(
    partial_ref, tok_ref, norm_ref, rg_ref, re_ref, routes_ref, gate_ref, up_ref, down_ref,
    out_ref,
    partial, tok, norm, rg, rex, routes, other, xm, moe,
    wg, wu, wd, sendc, recvc, send1, recv1, sendm, recvm, send2, recv2, part, partr, res, ret, comb, back,
    isem, wsem, w_ss, w_rs, xs, xr, scs, scr, s1s, s1r, sms, smr, s2s, s2r, ps, pr, s3s, s3r, s4s, s4r,
):
    seqs, half = out_ref.shape
    fh = gate_ref.shape[2]
    experts = re_ref.shape[1]
    groups = rg_ref.shape[0]
    e = lax.axis_index("ep")
    t = lax.axis_index("tp")
    z, y, x = e // NQ, lax.rem(e // NX, NY), lax.rem(e, NX)
    me_q = lax.rem(e, NQ)
    partner = (e, 1 - t)

    def z_peer(d):
        return lax.rem(z + d + NZ, NZ) * NQ + me_q

    def q_of(a, b):
        return lax.rem(y + a + NY, NY) * NX + lax.rem(x + b + NX, NX)

    plane = [(a, b) for a in range(NY) for b in range(NX) if a or b]

    barrier = pltpu.get_barrier_semaphore()
    pl.semaphore_signal(barrier, inc=1, device_id=partner, device_id_type=MESH)
    for d in range(1, NZ):
        pl.semaphore_signal(barrier, inc=1, device_id=(z_peer(d), t), device_id_type=MESH)
    for a, b in plane:
        pl.semaphore_signal(barrier, inc=1, device_id=(z * NQ + q_of(a, b), t), device_id_type=MESH)

    mine = pl.ds(pl.multiple_of(t * half, half), half)
    theirs = pl.ds(pl.multiple_of((1 - t) * half, half), half)
    lanes = pl.ds(pl.multiple_of(t * fh, fh), fh)
    local = [
        pltpu.make_async_copy(gate_ref.at[0, mine], wg.at[:, lanes], wsem.at[0]),
        pltpu.make_async_copy(up_ref.at[0, mine], wu.at[:, lanes], wsem.at[1]),
        pltpu.make_async_copy(down_ref.at[0, :, mine], wd.at[lanes], wsem.at[2]),
    ]
    loads = {}
    for i, (name, src, dst) in enumerate([
        ("routes", routes_ref, routes), ("partial", partial_ref, partial), ("tok", tok_ref, tok), ("norm", norm_ref, norm),
        ("rex", re_ref, rex), ("rg", rg_ref, rg),
    ]):
        loads[name] = pltpu.make_async_copy(src, dst, isem.at[i])
        loads[name].start()
    for copy in local:
        copy.start()

    loads["routes"].wait()
    table = jnp.concatenate([routes[...].astype(F32), jnp.zeros_like(routes, F32)], axis=0).astype(BF16)
    named = nt_dot(one_hot(iota((seqs, seqs), 0) == iota((seqs, seqs), 1)), table)
    expert_lane = iota((seqs, experts), 1).astype(F32)
    hit = jnp.zeros((seqs, experts), F32)
    for k in range(routes.shape[0]):
        hit += jnp.where(named[:, k : k + 1] == expert_lane, 1.0, 0.0)
    earlier = one_hot(iota((seqs, seqs), 1) < iota((seqs, seqs), 0))
    first = jnp.where(jnp.dot(earlier, hit.astype(BF16), preferred_element_type=F32) < 0.5, hit, 0.0)
    fold_row = iota((2 * experts, 128), 0)
    fold = one_hot(iota((2 * experts, 128), 1) == (fold_row // experts) * NQ + lax.rem(fold_row, NQ))
    group_of = one_hot(iota((experts, groups), 0) // (experts // groups) == iota((experts, groups), 1))
    in_group = jnp.where(jnp.dot(hit.astype(BF16), group_of, preferred_element_type=F32) > 0.5, 1.0, 0.0)
    before = jnp.dot(earlier, in_group.astype(BF16), preferred_element_type=F32)
    slot = jnp.sum(in_group * (4.0 * iota((seqs, groups), 1).astype(F32) + before), axis=1, keepdims=True)
    p1t = one_hot(slot == iota((seqs, 64), 1).astype(F32))
    p1 = nt_dot(one_hot(iota((64, 64), 0) == iota((64, 64), 1)), p1t).astype(BF16)
    ranked = jnp.concatenate([first, hit - first], axis=1)
    choice = jnp.dot(ranked.astype(BF16), fold, preferred_element_type=F32).astype(BF16)
    choice = jnp.dot(p1, choice, preferred_element_type=F32)
    for i in range(NZ):
        sendc[i] = choice[8 * i : 8 * i + 8].astype(BF16)

    loads["partial"].wait()
    pl.semaphore_wait(barrier, NZ + NQ - 1)

    def remote(src, dst, ss, rs, device):
        copy = pltpu.make_async_remote_copy(src, dst, ss, rs, device_id=device, device_id_type=MESH)
        copy.start()
        return copy

    def along_z(src, dst, ss, rs, step):
        return remote(src, dst, ss, rs, (z_peer(step), t))

    sent = [remote(partial, other, xs.at[0], xr.at[0], partner)]
    mixer_copy = sent[0]
    choices = []
    for p in range(1, NZ):
        zd = lax.rem(z + ORDER[p], NZ)
        choices.append(along_z(sendc.at[zd], recvc.at[p], scs.at[p], scr.at[p], ORDER[p]))
    recvc[0] = sendc[z]
    loads["tok"].wait()
    loads["norm"].wait()
    gain = norm[...].astype(F32).reshape(1, -1)
    mixer_copy.wait_recv()
    mixer_out = (partial[...] + other[...]).astype(BF16)
    x_mid = (tok[...].astype(F32) + mixer_out.astype(F32)).astype(BF16)
    moe_in = scale_rows(x_mid.astype(F32), gain)
    for i in range(2):
        xm[i] = x_mid[:, i * half : (i + 1) * half]
        moe[i] = moe_in[:, i * half : (i + 1) * half]
    rows = jnp.dot(p1, moe[t], preferred_element_type=F32)
    for i in range(NZ):
        send1[i] = rows[8 * i : 8 * i + 8].astype(BF16)

    hop1 = [None]
    for p in range(1, NZ):
        zd = lax.rem(z + ORDER[p], NZ)
        hop1.append(along_z(send1.at[zd], recv1.at[p], s1s.at[p], s1r.at[p], ORDER[p]))
    recv1[0] = send1[z]
    weights = [
        remote(gate_ref.at[0, theirs], wg.at[:, lanes], w_ss.at[0], w_rs.at[0], partner),
        remote(up_ref.at[0, theirs], wu.at[:, lanes], w_ss.at[1], w_rs.at[1], partner),
        remote(down_ref.at[0, :, theirs], wd.at[lanes], w_ss.at[2], w_rs.at[2], partner),
    ]

    picks = 2 * BATCH * NQ
    inputs = 8 * BATCH
    col = iota((picks, 128), 0)
    expand = one_hot(iota((picks, 128), 1) == lax.rem(col, 2) * NQ + col // (2 * BATCH))
    same_t = lax.rem(iota((picks, inputs), 0) // 2, BATCH) == iota((picks, inputs), 1) // 8
    same = lax.rem(iota((inputs, picks), 1) // 2, BATCH) == iota((inputs, picks), 0) // 8
    for copy in choices:
        copy.wait_recv()
    hop2 = []
    for b in range(2):
        group = slice(b * BATCH, (b + 1) * BATCH)
        chosen = recvc[group].astype(F32).reshape(inputs, 128).astype(BF16)
        choose = jnp.where(same_t, nt_dot(expand, chosen), 0.0).astype(BF16)
        for copy in hop1[group]:
            if copy is not None:
                copy.wait_recv()
        arrived = recv1[group].astype(F32).reshape(inputs, half).astype(BF16)
        picked = jnp.dot(choose, arrived, preferred_element_type=F32)
        send2[b] = picked.reshape(NQ, 2 * BATCH, half).astype(BF16)
        copies = []
        for i, (a, c) in enumerate(plane, 1):
            q = q_of(a, c)
            copies.append(remote(send2.at[b, q], recv2.at[b, i], s2s.at[b, i], s2r.at[b, i], (z * NQ + q, t)))
        recv2[b, 0] = send2[b, me_q]
        hop2.append(copies)
        if b == 0:
            loads["rex"].wait()
            loads["rg"].wait()
            scores = hit * sigmoid(jnp.dot(moe_in, rex[...], preferred_element_type=F32))
            group_prob = sigmoid(jnp.sum(in_group * nt_dot(moe_in, rg[...]), axis=1, keepdims=True))
            route_weight = group_prob * scores / jnp.sum(scores, axis=1, keepdims=True)
            weighed = jnp.concatenate([route_weight * first, route_weight * (hit - first)], axis=1)
            weighed = split_dot(weighed, fold)
            high = weighed.astype(BF16)
            low = (weighed - high.astype(F32)).astype(BF16)
            sendm[...] = (
                jnp.dot(p1, high, preferred_element_type=F32) + jnp.dot(p1, low, preferred_element_type=F32)
            ).reshape(NZ, 8, 128)
            hopw = []
            for p in range(1, NZ):
                zd = lax.rem(z + ORDER[p], NZ)
                hopw.append(along_z(sendm.at[zd], recvm.at[p], sms.at[p], smr.at[p], ORDER[p]))
            recvm[0] = sendm[z]

    for copy in hopw:
        copy.wait_recv()
    weigh = []
    for b in range(2):
        meta = recvm[b * BATCH : (b + 1) * BATCH].reshape(inputs, 128)
        meta_hi = meta.astype(BF16)
        meta_lo = (meta - meta_hi.astype(F32)).astype(BF16)
        for half_meta in (meta_hi, meta_lo):
            weigh.append(jnp.where(same, nt_dot(half_meta, expand), 0.0).astype(BF16))

    for copy in local:
        copy.wait()
    for copy in weights:
        copy.wait_recv()

    hop3 = []
    for b in range(2):
        for copy in hop2[b]:
            copy.wait_recv()
        flat = recv2[b].astype(F32).reshape(picks, half).astype(BF16)
        gate_part = jnp.dot(flat, wg[...], preferred_element_type=F32)
        part[b, 0] = gate_part.astype(BF16)
        gate_copy = remote(part.at[b, 0], partr.at[b, 0], ps.at[b, 0], pr.at[b, 0], partner)
        up_part = jnp.dot(flat, wu[...], preferred_element_type=F32)
        part[b, 1] = up_part.astype(BF16)
        up_copy = remote(part.at[b, 1], partr.at[b, 1], ps.at[b, 1], pr.at[b, 1], partner)
        sent += [gate_copy, up_copy]
        gate_copy.wait_recv()
        gate_sum = gate_part + partr[b, 0].astype(F32)
        gated = gate_sum * sigmoid(gate_sum)
        up_copy.wait_recv()
        hidden = (gated * (up_part + partr[b, 1].astype(F32))).astype(BF16)
        result = jnp.dot(hidden, wd[...], preferred_element_type=F32)
        res[b] = result.reshape(NQ, 2 * BATCH, half).astype(BF16)
        copies = []
        for i, (a, c) in enumerate(plane, 1):
            q = q_of(-a, -c)
            copies.append(remote(res.at[b, i], ret.at[b, me_q], s3s.at[b, i], s3r.at[b, i], (z * NQ + q, t)))
        ret[b, me_q] = res[b, 0]
        hop3.append(copies)

    hop4 = []
    for b in range(2):
        for copy in hop3[b]:
            copy.wait_recv()
        results = ret[b].astype(F32).reshape(picks, half).astype(BF16)
        summed = jnp.dot(weigh[2 * b], results, preferred_element_type=F32)
        summed += jnp.dot(weigh[2 * b + 1], results, preferred_element_type=F32)
        for k in range(BATCH):
            p = b * BATCH + k
            comb[p] = summed[8 * k : 8 * k + 8].astype(BF16)
        for k in range(BATCH):
            p = b * BATCH + k
            if p:
                hop4.append(along_z(comb.at[p], back.at[z], s4s.at[p], s4r.at[p], -ORDER[p]))
    back[z] = comb[0]
    for copy in hop4:
        copy.wait_recv()
    sums = back[...].astype(F32).reshape(64, half).astype(BF16)
    moe_out = jnp.dot(p1t, sums, preferred_element_type=F32)
    out_ref[...] = (xm[t].astype(F32) + moe_out).astype(BF16)

    for copy in sent + choices + hop1[1:] + hopw + weights + hop2[0] + hop2[1] + hop3[0] + hop3[1] + hop4:
        copy.wait_send()


def exchange(partial, tok, norm, rg, rex, routes, gate, up, down):
    seqs, half = tok.shape[0], tok.shape[1] // 2
    fh = gate.shape[2]
    hbm = pl.BlockSpec(memory_space=pl.ANY)
    dma = pltpu.SemaphoreType.DMA
    small = (partial, tok, norm, rg, rex, routes)
    by_half = pltpu.VMEM((2, seqs, half), BF16)
    by_z = pltpu.VMEM((NZ, 8, half), BF16)
    by_q = pltpu.VMEM((2, NQ, 2 * BATCH, half), BF16)
    parts = pltpu.VMEM((2, 2, 2 * BATCH * NQ, 2 * fh), BF16)
    return pl.pallas_call(
        exchange_kernel,
        out_shape=jax.ShapeDtypeStruct((seqs, half), BF16),
        in_specs=[hbm] * 9,
        out_specs=pl.BlockSpec(memory_space=pltpu.VMEM),
        scratch_shapes=[pltpu.VMEM(a.shape, a.dtype) for a in small]
        + [
            pltpu.VMEM(partial.shape, F32),
            by_half,
            by_half,
            pltpu.VMEM((half, 2 * fh), BF16),
            pltpu.VMEM((half, 2 * fh), BF16),
            pltpu.VMEM((2 * fh, half), BF16),
            pltpu.VMEM((NZ, 8, 128), BF16),
            pltpu.VMEM((NZ, 8, 128), BF16),
            by_z,
            by_z,
            pltpu.VMEM((NZ, 8, 128), F32),
            pltpu.VMEM((NZ, 8, 128), F32),
            by_q,
            by_q,
            parts,
            parts,
            by_q,
            by_q,
            by_z,
            by_z,
            dma((len(small),)),
            dma((3,)), dma((3,)), dma((3,)),
            dma((1,)), dma((1,)),
            dma((NZ,)), dma((NZ,)), dma((NZ,)), dma((NZ,)), dma((NZ,)), dma((NZ,)),
            dma((2, NQ)), dma((2, NQ)),
            dma((2, 2)), dma((2, 2)),
            dma((2, NQ)), dma((2, NQ)),
            dma((NZ,)), dma((NZ,)),
        ],
        compiler_params=pltpu.CompilerParams(
            collective_id=0, has_side_effects=True, vmem_limit_bytes=67043328
        ),
    )(*small, gate, up, down)


def shards(
    tokens_in, state_in, norm_mix, w_recept, w_key, w_value, decay_down, decay_up, decay_base,
    iclr_down, iclr_up, iclr_base, key_scale, key_mix, w_out, norm_moe, router_group,
    router_expert, routes, expert_gate, expert_up, expert_down,
):
    partial_value, state_out = front(
        tokens_in, norm_mix, w_recept, w_key, w_value, decay_down.T, decay_up, decay_base,
        iclr_down.T, iclr_up, iclr_base, key_scale, key_mix, w_out, state_in,
    )
    layer_out = exchange(
        partial_value, tokens_in, norm_moe, router_group.T, router_expert, routes.T,
        expert_gate, expert_up, expert_down,
    )
    return (layer_out, state_out)


def solution(mesh):
    in_specs = (
        P("ep", None),
        P("ep", "tp", None, None),
        P(),
        P(None, "tp"),
        P(None, "tp"),
        P(None, "tp"),
        P(),
        P(None, "tp"),
        P("tp"),
        P(),
        P(None, "tp"),
        P("tp"),
        P("tp"),
        P("tp"),
        P("tp", None),
        P(),
        P(),
        P(),
        P("ep", None),
        P("ep", None, "tp"),
        P("ep", None, "tp"),
        P("ep", "tp", None),
    )
    out_specs = (P("ep", "tp"), P("ep", "tp", None, None))
    return jax.shard_map(shards, mesh=mesh, in_specs=in_specs, out_specs=out_specs, check_vma=False)
```

```python
import math

import jax
import jax.numpy as jnp
from jax import lax
from jax.experimental import pallas as pl
from jax.experimental.pallas import tpu as pltpu
from jax.sharding import PartitionSpec as P

MESH = pl.DeviceIdType.MESH
F32 = jnp.float32
BF16 = jnp.bfloat16
NZ, NY, NX = 8, 4, 4
NQ = NY * NX
ORDER = (0, 1, 7, 2, 6, 3, 5, 4)
BATCH = NZ // 2
PIECE = 1
PER = BATCH // PIECE


def iota(shape, dim):
    return lax.broadcasted_iota(jnp.int32, shape, dim)


def wait_for(name, region, sem):
    with jax.named_scope(name):
        pltpu.make_async_copy(region, region, sem).wait()


def arrive(name, copies):
    with jax.named_scope(name):
        for copy in copies:
            copy.wait_recv()


def one_hot(where):
    return jnp.where(where, 1.0, 0.0).astype(BF16)


def nt_dot(a, b):
    return lax.dot_general(a, b, (((1,), (1,)), ((), ())), preferred_element_type=F32)


def scale_rows(values32, gain):
    mean = jnp.mean(values32 * values32, axis=-1, keepdims=True)
    return (values32 * lax.rsqrt(mean + 1e-06) * gain).astype(BF16)


def sigmoid(u):
    return 1.0 / (1.0 + jnp.exp(-u))


def split_dot(a, b):
    hi = a.astype(BF16)
    lo = (a - hi.astype(F32)).astype(BF16)
    return jnp.dot(hi, b, preferred_element_type=F32) + jnp.dot(lo, b, preferred_element_type=F32)


def front_kernel(
    tok_ref, norm_ref, wr_ref, wk_ref, wv_ref, dd_ref, du_ref, db_ref, id_ref, iu_ref, ib_ref,
    ks_ref, km_ref, wo_ref, state_ref,
    partial_ref, state_out_ref,
    tok, norm, wr, wk, wv, dd, du, db, idn, iu, ib, ks, km, wo, sin, sout, lhs, decay, tall,
    isem, ssem, osem,
):
    seqs, heads, hs, _ = state_ref.shape
    width = heads * hs
    chunk = 8
    chunks = seqs // chunk
    loads = {}
    order = [
        ("tok", tok_ref, tok), ("norm", norm_ref, norm), ("wk", wk_ref, wk), ("dd", dd_ref, dd), ("id", id_ref, idn),
        ("wv", wv_ref, wv), ("wr", wr_ref, wr), ("du", du_ref, du), ("db", db_ref, db), ("iu", iu_ref, iu),
        ("ib", ib_ref, ib), ("ks", ks_ref, ks), ("km", km_ref, km),
    ]
    for i, (name, src, dst) in enumerate(order):
        loads[name] = pltpu.make_async_copy(src, dst, isem.at[i])
        loads[name].start()
    states = []
    for c in range(chunks):
        rows = pl.ds(c * chunk, chunk)
        states.append(pltpu.make_async_copy(state_ref.at[rows], sin.at[rows], ssem.at[c]))
        states[c].start()
    loads["wo"] = pltpu.make_async_copy(wo_ref, wo, isem.at[len(order)])
    loads["wo"].start()

    def got(*names):
        for name in names:
            loads[name].wait()

    got("tok", "norm")
    normed = scale_rows(tok[...].astype(F32), norm[...].astype(F32).reshape(1, -1))

    def project(weight):
        return jnp.dot(normed, weight[...], preferred_element_type=F32).astype(BF16)

    got("wk")
    key = project(wk).astype(F32)
    got("dd", "id")
    decay_low = jnp.tanh(nt_dot(normed, dd[...])).astype(BF16)
    iclr_low = nt_dot(normed, idn[...]).astype(BF16)
    got("wv", "wr")
    value = project(wv)
    recept = project(wr)
    got("du", "db", "iu", "ib", "ks", "km")
    rate_in = db[...].reshape(1, -1) + jnp.dot(decay_low, du[...], preferred_element_type=F32)
    decays = jnp.exp(-math.exp(-0.5) * sigmoid(rate_in))
    learn = sigmoid(ib[...].reshape(1, -1) + jnp.dot(iclr_low, iu[...], preferred_element_type=F32))
    scaled = key * ks[...].astype(F32).reshape(1, -1)
    head_ones = jnp.where(iota((width, width), 0) // hs == iota((width, width), 1) // hs, 1.0, 0.0).astype(BF16)
    unit_key = scaled * lax.rsqrt(split_dot(scaled * scaled, head_ones) + 1e-06)
    key_mod = key * (1.0 + (learn - 1.0) * km[...].astype(F32).reshape(1, -1))

    def by_head(values):
        return jnp.concatenate([values[:, h * hs : (h + 1) * hs] for h in range(heads)], axis=0)

    pairs = heads * seqs
    decay[...] = by_head(decays)
    keys_u = by_head(unit_key).astype(BF16)
    right = jnp.concatenate([by_head(-unit_key * learn), by_head(key_mod)], axis=0).astype(BF16)
    reads = by_head(recept.astype(F32)).astype(BF16)
    pick = jnp.where(iota((seqs, pairs), 0) == lax.rem(iota((seqs, pairs), 1), seqs), 1.0, 0.0).astype(BF16)
    spread = lax.dot_general(value, pick, (((0,), (0,)), ((), ())), preferred_element_type=F32)

    lane = iota((hs, pairs), 1)
    tall[...] = jnp.zeros_like(tall)
    for c in range(chunks):
        states[c].wait()
        for s in range(c * chunk, (c + 1) * chunk):
            found = nt_dot(sin[s].reshape(width, hs).astype(BF16), keys_u)
            for h in range(heads):
                own = lane == h * seqs + s
                rows = slice(h * hs, (h + 1) * hs)
                lhs[s - c * chunk, rows, :pairs] = jnp.where(own, found[rows], 0.0).astype(BF16)
                lhs[s - c * chunk, rows, pairs:] = jnp.where(own, spread[rows], 0.0).astype(BF16)
        for s in range(c * chunk, (c + 1) * chunk):
            update = jnp.dot(lhs[s - c * chunk], right, preferred_element_type=F32)
            for h in range(heads):
                row = h * seqs + s
                sout[s, h] = sin[s, h] * decay[row : row + 1, :] + update[h * hs : (h + 1) * hs]
        rows = pl.ds(c * chunk, chunk)
        pltpu.make_async_copy(sout.at[rows], state_out_ref.at[rows], osem.at[c]).start()
        for s in range(c * chunk, (c + 1) * chunk):
            seen = nt_dot(sout[s].reshape(width, hs).astype(BF16), reads)
            for h in range(heads):
                rows = slice(h * hs, (h + 1) * hs)
                tall[rows] = jnp.where(lane == h * seqs + s, seen[rows], tall[rows])
    mixed = nt_dot(pick, tall[...].astype(BF16)).astype(BF16)
    got("wo")
    partial_ref[...] = jnp.dot(mixed, wo[...], preferred_element_type=F32)
    for c in range(chunks):
        rows = pl.ds(c * chunk, chunk)
        pltpu.make_async_copy(sout.at[rows], state_out_ref.at[rows], osem.at[c]).wait()


def front(tok, norm, wr, wk, wv, dd, du, db, idn, iu, ib, ks, km, wo, state):
    seqs, heads, hs, _ = state.shape
    width, pairs = heads * hs, heads * seqs
    hbm = pl.BlockSpec(memory_space=pltpu.HBM)
    args = (tok, norm, wr, wk, wv, dd, du, db, idn, iu, ib, ks, km, wo)
    return pl.pallas_call(
        front_kernel,
        out_shape=(
            jax.ShapeDtypeStruct(tok.shape, F32),
            jax.ShapeDtypeStruct(state.shape, F32),
        ),
        in_specs=[hbm] * 15,
        out_specs=(pl.BlockSpec(memory_space=pltpu.VMEM), hbm),
        scratch_shapes=[pltpu.VMEM(a.shape, a.dtype) for a in args]
        + [
            pltpu.VMEM(state.shape, F32),
            pltpu.VMEM(state.shape, F32),
            pltpu.VMEM((8, width, 2 * pairs), BF16),
            pltpu.VMEM((pairs, hs), F32),
            pltpu.VMEM((width, pairs), F32),
            pltpu.SemaphoreType.DMA((len(args),)),
            pltpu.SemaphoreType.DMA((seqs // 8,)),
            pltpu.SemaphoreType.DMA((seqs // 8,)),
        ],
        compiler_params=pltpu.CompilerParams(vmem_limit_bytes=67043328),
    )(*args, state)


def exchange_kernel(
    partial_ref, tok_ref, norm_ref, rg_ref, re_ref, routes_ref, gate_ref, up_ref, down_ref,
    out_ref,
    partial, tok, norm, rg, rex, routes, other, xm, moe,
    wg, wu, wd, sendc, recvc, send1, recv1, sendm, recvm, send2, recv2, part, partr, res, ret, comb, back,
    isem, wsem, w_ss, w_rs, xs, xr, scs, scr, s1s, s1r, sms, smr, s2s, s2r, ps, pr, s3s, s3r, s4s, s4r,
):
    seqs, half = out_ref.shape
    fh = gate_ref.shape[2]
    experts = re_ref.shape[1]
    groups = rg_ref.shape[0]
    e = lax.axis_index("ep")
    t = lax.axis_index("tp")
    z, y, x = e // NQ, lax.rem(e // NX, NY), lax.rem(e, NX)
    me_q = lax.rem(e, NQ)
    partner = (e, 1 - t)

    def z_peer(d):
        return lax.rem(z + d + NZ, NZ) * NQ + me_q

    def q_of(a, b):
        return lax.rem(y + a + NY, NY) * NX + lax.rem(x + b + NX, NX)

    plane = [(a, b) for a in range(NY) for b in range(NX) if a or b]

    barrier = pltpu.get_barrier_semaphore()
    pl.semaphore_signal(barrier, inc=1, device_id=partner, device_id_type=MESH)
    for d in range(1, NZ):
        pl.semaphore_signal(barrier, inc=1, device_id=(z_peer(d), t), device_id_type=MESH)
    for a, b in plane:
        pl.semaphore_signal(barrier, inc=1, device_id=(z * NQ + q_of(a, b), t), device_id_type=MESH)

    mine = pl.ds(pl.multiple_of(t * half, half), half)
    theirs = pl.ds(pl.multiple_of((1 - t) * half, half), half)
    lanes = pl.ds(pl.multiple_of(t * fh, fh), fh)
    local = [
        pltpu.make_async_copy(gate_ref.at[0, mine], wg.at[:, lanes], wsem.at[0]),
        pltpu.make_async_copy(up_ref.at[0, mine], wu.at[:, lanes], wsem.at[1]),
        pltpu.make_async_copy(down_ref.at[0, :, mine], wd.at[lanes], wsem.at[2]),
    ]
    loads = {}
    for i, (name, src, dst) in enumerate([
        ("partial", partial_ref, partial), ("routes", routes_ref, routes), ("tok", tok_ref, tok), ("norm", norm_ref, norm),
        ("rex", re_ref, rex), ("rg", rg_ref, rg),
    ]):
        loads[name] = pltpu.make_async_copy(src, dst, isem.at[i])
        loads[name].start()
    for copy in local:
        copy.start()

    with jax.named_scope("enter"):
        loads["partial"].wait()
        pl.semaphore_wait(barrier, NZ + NQ - 1)

    def remote(src, dst, ss, rs, device):
        copy = pltpu.make_async_remote_copy(src, dst, ss, rs, device_id=device, device_id_type=MESH)
        copy.start()
        return copy

    def along_z(src, dst, ss, rs, step):
        return remote(src, dst, ss, rs, (z_peer(step), t))

    sent = [remote(partial, other, xs.at[0], xr.at[0], partner)]
    mixer_copy = sent[0]
    loads["routes"].wait()
    table = jnp.concatenate([routes[...].astype(F32), jnp.zeros_like(routes, F32)], axis=0).astype(BF16)
    named = nt_dot(one_hot(iota((seqs, seqs), 0) == iota((seqs, seqs), 1)), table)
    expert_lane = iota((seqs, experts), 1).astype(F32)
    hit = jnp.zeros((seqs, experts), F32)
    for k in range(routes.shape[0]):
        hit += jnp.where(named[:, k : k + 1] == expert_lane, 1.0, 0.0)
    earlier = one_hot(iota((seqs, seqs), 1) < iota((seqs, seqs), 0))
    first = jnp.where(jnp.dot(earlier, hit.astype(BF16), preferred_element_type=F32) < 0.5, hit, 0.0)
    fold_row = iota((2 * experts, 128), 0)
    fold = one_hot(iota((2 * experts, 128), 1) == (fold_row // experts) * NQ + lax.rem(fold_row, NQ))
    group_of = one_hot(iota((experts, groups), 0) // (experts // groups) == iota((experts, groups), 1))
    in_group = jnp.where(jnp.dot(hit.astype(BF16), group_of, preferred_element_type=F32) > 0.5, 1.0, 0.0)
    before = jnp.dot(earlier, in_group.astype(BF16), preferred_element_type=F32)
    slot = jnp.sum(in_group * (4.0 * iota((seqs, groups), 1).astype(F32) + before), axis=1, keepdims=True)
    p1t = one_hot(slot == iota((seqs, 64), 1).astype(F32))
    p1 = nt_dot(one_hot(iota((64, 64), 0) == iota((64, 64), 1)), p1t).astype(BF16)
    ranked = jnp.concatenate([first, hit - first], axis=1)
    choice = jnp.dot(ranked.astype(BF16), fold, preferred_element_type=F32).astype(BF16)
    choice = jnp.dot(p1, choice, preferred_element_type=F32)
    for i in range(NZ):
        sendc[i] = choice[8 * i : 8 * i + 8].astype(BF16)

    for p in range(1, NZ):
        zd = lax.rem(z + ORDER[p], NZ)
        along_z(sendc.at[zd], recvc.at[p], scs, scr.at[p // PIECE], ORDER[p])
    recvc[0] = sendc[z]
    loads["tok"].wait()
    loads["norm"].wait()
    gain = norm[...].astype(F32).reshape(1, -1)
    arrive("mixer", [mixer_copy])
    mixer_out = (partial[...] + other[...]).astype(BF16)
    x_mid = (tok[...].astype(F32) + mixer_out.astype(F32)).astype(BF16)
    moe_in = scale_rows(x_mid.astype(F32), gain)
    for i in range(2):
        xm[i] = x_mid[:, i * half : (i + 1) * half]
        moe[i] = moe_in[:, i * half : (i + 1) * half]
    rows = jnp.dot(p1, moe[t], preferred_element_type=F32)
    for i in range(NZ):
        send1[i] = rows[8 * i : 8 * i + 8].astype(BF16)

    for p in range(1, NZ):
        zd = lax.rem(z + ORDER[p], NZ)
        along_z(send1.at[zd], recv1.at[p], s1s, s1r.at[p // PIECE], ORDER[p])
    recv1[0] = send1[z]
    weights = [
        remote(gate_ref.at[0, theirs], wg.at[:, lanes], w_ss.at[0], w_rs.at[0], partner),
        remote(up_ref.at[0, theirs], wu.at[:, lanes], w_ss.at[1], w_rs.at[1], partner),
        remote(down_ref.at[0, :, theirs], wd.at[lanes], w_ss.at[2], w_rs.at[2], partner),
    ]

    picks = 2 * PIECE * NQ
    inputs = 8 * PIECE
    col = iota((picks, 128), 0)
    expand = one_hot(iota((picks, 128), 1) == lax.rem(col, 2) * NQ + col // (2 * PIECE))
    same = lax.rem(iota((picks, inputs), 0) // 2, PIECE) == iota((picks, inputs), 1) // 8
    for g in range(NZ // PIECE):
        group = slice(g * PIECE, (g + 1) * PIECE)
        came = pl.ds(max(1, g * PIECE), (g + 1) * PIECE - max(1, g * PIECE))
        if came.size:
            wait_for("choices", recvc.at[came], scr.at[g])
        chosen = recvc[group].astype(F32).reshape(inputs, 128).astype(BF16)
        choose = jnp.where(same, nt_dot(expand, chosen), 0.0).astype(BF16)
        if came.size:
            wait_for("hop1", recv1.at[came], s1r.at[g])
        arrived = recv1[group].astype(F32).reshape(inputs, half).astype(BF16)
        picked = jnp.dot(choose, arrived, preferred_element_type=F32)
        send2[g] = picked.reshape(NQ, 2 * PIECE, half).astype(BF16)
        for i, (a, c) in enumerate(plane, 1):
            q = q_of(a, c)
            remote(send2.at[g, q], recv2.at[g, i], s2s, s2r.at[g // PER], (z * NQ + q, t))
        recv2[g, 0] = send2[g, me_q]

    loads["rex"].wait()
    loads["rg"].wait()
    scores = hit * sigmoid(jnp.dot(moe_in, rex[...], preferred_element_type=F32))
    group_prob = sigmoid(jnp.sum(in_group * nt_dot(moe_in, rg[...]), axis=1, keepdims=True))
    route_weight = group_prob * scores / jnp.sum(scores, axis=1, keepdims=True)
    weighed = jnp.concatenate([route_weight * first, route_weight * (hit - first)], axis=1)
    weighed = split_dot(weighed, fold)
    high = weighed.astype(BF16)
    low = (weighed - high.astype(F32)).astype(BF16)
    sendm[...] = (
        jnp.dot(p1, high, preferred_element_type=F32) + jnp.dot(p1, low, preferred_element_type=F32)
    ).reshape(NZ, 8, 128)
    for p in range(1, NZ):
        zd = lax.rem(z + ORDER[p], NZ)
        along_z(sendm.at[zd], recvm.at[p], sms, smr, ORDER[p])
    recvm[0] = sendm[z]

    for copy in local:
        copy.wait()
    arrive("experts", weights)

    for b in range(2):
        wait_for("hop2", recv2.at[pl.ds(b * PER, PER), pl.ds(1, NQ - 1)], s2r.at[b])
        flat = recv2[b * PER : (b + 1) * PER].astype(F32).reshape(PER * picks, half).astype(BF16)
        gate_part = jnp.dot(flat, wg[...], preferred_element_type=F32)
        part[b, 0] = gate_part.astype(BF16)
        gate_copy = remote(part.at[b, 0], partr.at[b, 0], ps, pr.at[b, 0], partner)
        up_part = jnp.dot(flat, wu[...], preferred_element_type=F32)
        part[b, 1] = up_part.astype(BF16)
        up_copy = remote(part.at[b, 1], partr.at[b, 1], ps, pr.at[b, 1], partner)
        arrive("gate", [gate_copy])
        gate_sum = gate_part + partr[b, 0].astype(F32)
        gated = gate_sum * sigmoid(gate_sum)
        arrive("up", [up_copy])
        hidden = (gated * (up_part + partr[b, 1].astype(F32))).astype(BF16)
        result = jnp.dot(hidden, wd[...], preferred_element_type=F32)
        res[b] = result.reshape(PER, NQ, 2 * PIECE, half).astype(BF16)
        for i, (a, c) in enumerate(plane, 1):
            q = q_of(-a, -c)
            remote(res.at[b, :, i], ret.at[b, :, me_q], s3s, s3r.at[b], (z * NQ + q, t))
        for g in range(PER):
            ret[b, g, me_q] = res[b, g, 0]

    wait_for("weights", recvm.at[pl.ds(1, NZ - 1)], smr)
    row = iota((8 * BATCH, PER * picks), 0) // 8
    column = iota((8 * BATCH, PER * picks), 1)
    own = row == column // picks * PIECE + lax.rem(column // 2, PIECE)
    weigh = []
    for b in range(2):
        meta = recvm[b * BATCH : (b + 1) * BATCH].reshape(8 * BATCH, 128)
        meta_hi = meta.astype(BF16)
        meta_lo = (meta - meta_hi.astype(F32)).astype(BF16)
        for half_meta in (meta_hi, meta_lo):
            spread = nt_dot(half_meta, expand)
            weigh.append(jnp.where(own, jnp.concatenate([spread] * PER, axis=1), 0.0).astype(BF16))

    for b in range(2):
        wait_for("hop3", ret.at[b, :, pl.ds(1, NQ - 1)], s3r.at[b])
        results = ret[b].astype(F32).reshape(PER * picks, half).astype(BF16)
        summed = jnp.dot(weigh[2 * b], results, preferred_element_type=F32)
        summed += jnp.dot(weigh[2 * b + 1], results, preferred_element_type=F32)
        for k in range(BATCH):
            p = b * BATCH + k
            comb[p] = summed[8 * k : 8 * k + 8].astype(BF16)
        for k in range(BATCH):
            p = b * BATCH + k
            if p:
                along_z(comb.at[p], back.at[z], s4s, s4r, -ORDER[p])
    back[z] = comb[0]
    wait_for("hop4", back.at[pl.ds(1, NZ - 1)], s4r)
    sums = back[...].astype(F32).reshape(64, half).astype(BF16)
    moe_out = jnp.dot(p1t, sums, preferred_element_type=F32)
    out_ref[...] = (xm[t].astype(F32) + moe_out).astype(BF16)

    for copy in sent + weights:
        copy.wait_send()
    others = pl.ds(1, NZ - 1)
    for region, sem in (
        (sendc.at[others], scs), (send1.at[others], s1s), (sendm.at[others], sms), (comb.at[others], s4s),
        (send2.at[:, pl.ds(1, NQ - 1)], s2s), (part, ps), (res.at[:, :, pl.ds(1, NQ - 1)], s3s),
    ):
        wait_for("sent", region, sem)


def exchange(partial, tok, norm, rg, rex, routes, gate, up, down):
    seqs, half = tok.shape[0], tok.shape[1] // 2
    fh = gate.shape[2]
    hbm = pl.BlockSpec(memory_space=pl.ANY)
    dma = pltpu.SemaphoreType.DMA
    small = (partial, tok, norm, rg, rex, routes)
    by_half = pltpu.VMEM((2, seqs, half), BF16)
    by_z = pltpu.VMEM((NZ, 8, half), BF16)
    pieces = NZ // PIECE
    in_q = pltpu.VMEM((pieces, NQ, 2 * PIECE, half), BF16)
    out_q = pltpu.VMEM((2, PER, NQ, 2 * PIECE, half), BF16)
    parts = pltpu.VMEM((2, 2, 2 * BATCH * NQ, 2 * fh), BF16)
    return pl.pallas_call(
        exchange_kernel,
        out_shape=jax.ShapeDtypeStruct((seqs, half), BF16),
        in_specs=[hbm] * 9,
        out_specs=pl.BlockSpec(memory_space=pltpu.VMEM),
        scratch_shapes=[pltpu.VMEM(a.shape, a.dtype) for a in small]
        + [
            pltpu.VMEM(partial.shape, F32),
            by_half,
            by_half,
            pltpu.VMEM((half, 2 * fh), BF16),
            pltpu.VMEM((half, 2 * fh), BF16),
            pltpu.VMEM((2 * fh, half), BF16),
            pltpu.VMEM((NZ, 8, 128), BF16),
            pltpu.VMEM((NZ, 8, 128), BF16),
            by_z,
            by_z,
            pltpu.VMEM((NZ, 8, 128), F32),
            pltpu.VMEM((NZ, 8, 128), F32),
            in_q,
            in_q,
            parts,
            parts,
            out_q,
            out_q,
            by_z,
            by_z,
            dma((len(small),)),
            dma((3,)), dma((3,)), dma((3,)),
            dma((1,)), dma((1,)),
            dma, dma((pieces,)), dma, dma((pieces,)), dma, dma,
            dma, dma((2,)),
            dma, dma((2, 2)),
            dma, dma((2,)),
            dma, dma,
        ],
        compiler_params=pltpu.CompilerParams(
            collective_id=0, has_side_effects=True, vmem_limit_bytes=67043328
        ),
    )(*small, gate, up, down)


def shards(
    tokens_in, state_in, norm_mix, w_recept, w_key, w_value, decay_down, decay_up, decay_base,
    iclr_down, iclr_up, iclr_base, key_scale, key_mix, w_out, norm_moe, router_group,
    router_expert, routes, expert_gate, expert_up, expert_down,
):
    partial_value, state_out = front(
        tokens_in, norm_mix, w_recept, w_key, w_value, decay_down.T, decay_up, decay_base,
        iclr_down.T, iclr_up, iclr_base, key_scale, key_mix, w_out, state_in,
    )
    layer_out = exchange(
        partial_value, tokens_in, norm_moe, router_group.T, router_expert, routes.T,
        expert_gate, expert_up, expert_down,
    )
    return (layer_out, state_out)


def solution(mesh):
    in_specs = (
        P("ep", None),
        P("ep", "tp", None, None),
        P(),
        P(None, "tp"),
        P(None, "tp"),
        P(None, "tp"),
        P(),
        P(None, "tp"),
        P("tp"),
        P(),
        P(None, "tp"),
        P("tp"),
        P("tp"),
        P("tp"),
        P("tp", None),
        P(),
        P(),
        P(),
        P("ep", None),
        P("ep", None, "tp"),
        P("ep", None, "tp"),
        P("ep", "tp", None),
    )
    out_specs = (P("ep", "tp"), P("ep", "tp", None, None))
    return jax.shard_map(shards, mesh=mesh, in_specs=in_specs, out_specs=out_specs, check_vma=False)
```

```python
import math

import jax
import jax.numpy as jnp
from jax import lax
from jax.experimental import pallas as pl
from jax.experimental.pallas import tpu as pltpu
from jax.sharding import PartitionSpec as P

MESH = pl.DeviceIdType.MESH
F32 = jnp.float32
BF16 = jnp.bfloat16
NZ, NY, NX = 8, 4, 4
NQ = NY * NX
ORDER = (0, 1, 7, 2, 6, 3, 5, 4)
PASSES = ((0, 2), (2, 4), (4, 6), (6, 8))
FLIGHT = 1
PASS_OF = tuple(k for k, (low, high) in enumerate(PASSES) for _ in range(low, high))


def iota(shape, dim):
    return lax.broadcasted_iota(jnp.int32, shape, dim)


def wait_for(name, region, sem):
    with jax.named_scope(name):
        pltpu.make_async_copy(region, region, sem).wait()


def arrive(name, copies):
    with jax.named_scope(name):
        for copy in copies:
            copy.wait_recv()


def one_hot(where):
    return jnp.where(where, 1.0, 0.0).astype(BF16)


def nt_dot(a, b):
    return lax.dot_general(a, b, (((1,), (1,)), ((), ())), preferred_element_type=F32)


def scale_rows(values32, gain):
    mean = jnp.mean(values32 * values32, axis=-1, keepdims=True)
    return (values32 * lax.rsqrt(mean + 1e-06) * gain).astype(BF16)


def sigmoid(u):
    return 1.0 / (1.0 + jnp.exp(-u))


def split_dot(a, b):
    hi = a.astype(BF16)
    lo = (a - hi.astype(F32)).astype(BF16)
    return jnp.dot(hi, b, preferred_element_type=F32) + jnp.dot(lo, b, preferred_element_type=F32)


def front_kernel(
    tok_ref, norm_ref, wr_ref, wk_ref, wv_ref, dd_ref, du_ref, db_ref, id_ref, iu_ref, ib_ref,
    ks_ref, km_ref, wo_ref, state_ref,
    partial_ref, state_out_ref,
    tok, norm, wr, wk, wv, dd, du, db, idn, iu, ib, ks, km, wo, sin, sout, lhs, decay, tall,
    isem, ssem, osem,
):
    seqs, heads, hs, _ = state_ref.shape
    width = heads * hs
    chunk = 8
    chunks = seqs // chunk
    loads = {}
    order = [
        ("tok", tok_ref, tok), ("norm", norm_ref, norm), ("wk", wk_ref, wk), ("dd", dd_ref, dd), ("id", id_ref, idn),
        ("wv", wv_ref, wv), ("wr", wr_ref, wr), ("du", du_ref, du), ("db", db_ref, db), ("iu", iu_ref, iu),
        ("ib", ib_ref, ib), ("ks", ks_ref, ks), ("km", km_ref, km),
    ]
    for i, (name, src, dst) in enumerate(order):
        loads[name] = pltpu.make_async_copy(src, dst, isem.at[i])
        loads[name].start()
    states = []
    for c in range(chunks):
        rows = pl.ds(c * chunk, chunk)
        states.append(pltpu.make_async_copy(state_ref.at[rows], sin.at[rows], ssem.at[c]))
        states[c].start()
    loads["wo"] = pltpu.make_async_copy(wo_ref, wo, isem.at[len(order)])
    loads["wo"].start()

    def got(*names):
        for name in names:
            loads[name].wait()

    got("tok", "norm")
    normed = scale_rows(tok[...].astype(F32), norm[...].astype(F32).reshape(1, -1))

    def project(weight):
        return jnp.dot(normed, weight[...], preferred_element_type=F32).astype(BF16)

    got("wk")
    key = project(wk).astype(F32)
    got("dd", "id")
    decay_low = jnp.tanh(nt_dot(normed, dd[...])).astype(BF16)
    iclr_low = nt_dot(normed, idn[...]).astype(BF16)
    got("wv", "wr")
    value = project(wv)
    recept = project(wr)
    got("du", "db", "iu", "ib", "ks", "km")
    rate_in = db[...].reshape(1, -1) + jnp.dot(decay_low, du[...], preferred_element_type=F32)
    decays = jnp.exp(-math.exp(-0.5) * sigmoid(rate_in))
    learn = sigmoid(ib[...].reshape(1, -1) + jnp.dot(iclr_low, iu[...], preferred_element_type=F32))
    scaled = key * ks[...].astype(F32).reshape(1, -1)
    head_ones = jnp.where(iota((width, width), 0) // hs == iota((width, width), 1) // hs, 1.0, 0.0).astype(BF16)
    unit_key = scaled * lax.rsqrt(split_dot(scaled * scaled, head_ones) + 1e-06)
    key_mod = key * (1.0 + (learn - 1.0) * km[...].astype(F32).reshape(1, -1))

    def by_head(values):
        return jnp.concatenate([values[:, h * hs : (h + 1) * hs] for h in range(heads)], axis=0)

    pairs = heads * seqs
    decay[...] = by_head(decays)
    keys_u = by_head(unit_key).astype(BF16)
    right = jnp.concatenate([by_head(-unit_key * learn), by_head(key_mod)], axis=0).astype(BF16)
    reads = by_head(recept.astype(F32)).astype(BF16)
    pick = jnp.where(iota((seqs, pairs), 0) == lax.rem(iota((seqs, pairs), 1), seqs), 1.0, 0.0).astype(BF16)
    spread = lax.dot_general(value, pick, (((0,), (0,)), ((), ())), preferred_element_type=F32)

    lane = iota((hs, pairs), 1)
    tall[...] = jnp.zeros_like(tall)
    for c in range(chunks):
        states[c].wait()
        for s in range(c * chunk, (c + 1) * chunk):
            found = nt_dot(sin[s].reshape(width, hs).astype(BF16), keys_u)
            for h in range(heads):
                own = lane == h * seqs + s
                rows = slice(h * hs, (h + 1) * hs)
                lhs[s - c * chunk, rows, :pairs] = jnp.where(own, found[rows], 0.0).astype(BF16)
                lhs[s - c * chunk, rows, pairs:] = jnp.where(own, spread[rows], 0.0).astype(BF16)
        for s in range(c * chunk, (c + 1) * chunk):
            update = jnp.dot(lhs[s - c * chunk], right, preferred_element_type=F32)
            for h in range(heads):
                row = h * seqs + s
                sout[s, h] = sin[s, h] * decay[row : row + 1, :] + update[h * hs : (h + 1) * hs]
        rows = pl.ds(c * chunk, chunk)
        pltpu.make_async_copy(sout.at[rows], state_out_ref.at[rows], osem.at[c]).start()
        for s in range(c * chunk, (c + 1) * chunk):
            seen = nt_dot(sout[s].reshape(width, hs).astype(BF16), reads)
            for h in range(heads):
                rows = slice(h * hs, (h + 1) * hs)
                tall[rows] = jnp.where(lane == h * seqs + s, seen[rows], tall[rows])
    mixed = nt_dot(pick, tall[...].astype(BF16)).astype(BF16)
    got("wo")
    partial_ref[...] = jnp.dot(mixed, wo[...], preferred_element_type=F32)
    for c in range(chunks):
        rows = pl.ds(c * chunk, chunk)
        pltpu.make_async_copy(sout.at[rows], state_out_ref.at[rows], osem.at[c]).wait()


def front(tok, norm, wr, wk, wv, dd, du, db, idn, iu, ib, ks, km, wo, state):
    seqs, heads, hs, _ = state.shape
    width, pairs = heads * hs, heads * seqs
    hbm = pl.BlockSpec(memory_space=pltpu.HBM)
    args = (tok, norm, wr, wk, wv, dd, du, db, idn, iu, ib, ks, km, wo)
    return pl.pallas_call(
        front_kernel,
        out_shape=(
            jax.ShapeDtypeStruct(tok.shape, F32),
            jax.ShapeDtypeStruct(state.shape, F32),
        ),
        in_specs=[hbm] * 15,
        out_specs=(pl.BlockSpec(memory_space=pltpu.VMEM), hbm),
        scratch_shapes=[pltpu.VMEM(a.shape, a.dtype) for a in args]
        + [
            pltpu.VMEM(state.shape, F32),
            pltpu.VMEM(state.shape, F32),
            pltpu.VMEM((8, width, 2 * pairs), BF16),
            pltpu.VMEM((pairs, hs), F32),
            pltpu.VMEM((width, pairs), F32),
            pltpu.SemaphoreType.DMA((len(args),)),
            pltpu.SemaphoreType.DMA((seqs // 8,)),
            pltpu.SemaphoreType.DMA((seqs // 8,)),
        ],
        compiler_params=pltpu.CompilerParams(vmem_limit_bytes=67043328),
    )(*args, state)


def exchange_kernel(
    partial_ref, tok_ref, norm_ref, rg_ref, re_ref, routes_ref, gate_ref, up_ref, down_ref,
    out_ref,
    partial, tok, norm, rg, rex, routes, other, xm, moe,
    wg, wu, wd, sendc, recvc, send1, recv1, sendm, recvm, send2, recv2, part, partr, res, ret, comb, back,
    isem, wsem, w_ss, w_rs, xs, xr, scs, scr, s1s, s1r, sms, smr, s2s, s2r, ps, pr, s3s, s3r, s4s, s4r,
):
    seqs, half = out_ref.shape
    fh = gate_ref.shape[2]
    experts = re_ref.shape[1]
    groups = rg_ref.shape[0]
    e = lax.axis_index("ep")
    t = lax.axis_index("tp")
    z, y, x = e // NQ, lax.rem(e // NX, NY), lax.rem(e, NX)
    me_q = lax.rem(e, NQ)
    partner = (e, 1 - t)

    def z_peer(d):
        return lax.rem(z + d + NZ, NZ) * NQ + me_q

    def q_of(a, b):
        return lax.rem(y + a + NY, NY) * NX + lax.rem(x + b + NX, NX)

    plane = [(a, b) for a in range(NY) for b in range(NX) if a or b]

    barrier = pltpu.get_barrier_semaphore()
    pl.semaphore_signal(barrier, inc=1, device_id=partner, device_id_type=MESH)
    for d in range(1, NZ):
        pl.semaphore_signal(barrier, inc=1, device_id=(z_peer(d), t), device_id_type=MESH)
    for a, b in plane:
        pl.semaphore_signal(barrier, inc=1, device_id=(z * NQ + q_of(a, b), t), device_id_type=MESH)

    mine = pl.ds(pl.multiple_of(t * half, half), half)
    theirs = pl.ds(pl.multiple_of((1 - t) * half, half), half)
    lanes = pl.ds(pl.multiple_of(t * fh, fh), fh)
    local = [
        pltpu.make_async_copy(gate_ref.at[0, mine], wg.at[:, lanes], wsem.at[0]),
        pltpu.make_async_copy(up_ref.at[0, mine], wu.at[:, lanes], wsem.at[1]),
        pltpu.make_async_copy(down_ref.at[0, :, mine], wd.at[lanes], wsem.at[2]),
    ]
    loads = {}
    for i, (name, src, dst) in enumerate([
        ("partial", partial_ref, partial), ("routes", routes_ref, routes), ("tok", tok_ref, tok), ("norm", norm_ref, norm),
        ("rex", re_ref, rex), ("rg", rg_ref, rg),
    ]):
        loads[name] = pltpu.make_async_copy(src, dst, isem.at[i])
        loads[name].start()
    for copy in local:
        copy.start()

    with jax.named_scope("enter"):
        loads["partial"].wait()
        pl.semaphore_wait(barrier, NZ + NQ - 1)

    def remote(src, dst, ss, rs, device):
        copy = pltpu.make_async_remote_copy(src, dst, ss, rs, device_id=device, device_id_type=MESH)
        copy.start()
        return copy

    def along_z(src, dst, ss, rs, step):
        return remote(src, dst, ss, rs, (z_peer(step), t))

    sent = [remote(partial, other, xs.at[0], xr.at[0], partner)]
    mixer_copy = sent[0]
    loads["routes"].wait()
    table = jnp.concatenate([routes[...].astype(F32), jnp.zeros_like(routes, F32)], axis=0).astype(BF16)
    named = nt_dot(one_hot(iota((seqs, seqs), 0) == iota((seqs, seqs), 1)), table)
    expert_lane = iota((seqs, experts), 1).astype(F32)
    hit = jnp.zeros((seqs, experts), F32)
    for k in range(routes.shape[0]):
        hit += jnp.where(named[:, k : k + 1] == expert_lane, 1.0, 0.0)
    earlier = one_hot(iota((seqs, seqs), 1) < iota((seqs, seqs), 0))
    first = jnp.where(jnp.dot(earlier, hit.astype(BF16), preferred_element_type=F32) < 0.5, hit, 0.0)
    fold_row = iota((2 * experts, 128), 0)
    fold = one_hot(iota((2 * experts, 128), 1) == (fold_row // experts) * NQ + lax.rem(fold_row, NQ))
    group_of = one_hot(iota((experts, groups), 0) // (experts // groups) == iota((experts, groups), 1))
    in_group = jnp.where(jnp.dot(hit.astype(BF16), group_of, preferred_element_type=F32) > 0.5, 1.0, 0.0)
    before = jnp.dot(earlier, in_group.astype(BF16), preferred_element_type=F32)
    slot = jnp.sum(in_group * (4.0 * iota((seqs, groups), 1).astype(F32) + before), axis=1, keepdims=True)
    p1t = one_hot(slot == iota((seqs, 64), 1).astype(F32))
    p1 = nt_dot(one_hot(iota((64, 64), 0) == iota((64, 64), 1)), p1t).astype(BF16)
    ranked = jnp.concatenate([first, hit - first], axis=1)
    choice = jnp.dot(ranked.astype(BF16), fold, preferred_element_type=F32).astype(BF16)
    choice = jnp.dot(p1, choice, preferred_element_type=F32)
    for i in range(NZ):
        sendc[i] = choice[8 * i : 8 * i + 8].astype(BF16)

    for p in range(1, NZ):
        zd = lax.rem(z + ORDER[p], NZ)
        along_z(sendc.at[zd], recvc.at[p], scs, scr.at[p], ORDER[p])
    recvc[0] = sendc[z]
    loads["tok"].wait()
    loads["norm"].wait()
    gain = norm[...].astype(F32).reshape(1, -1)
    arrive("mixer", [mixer_copy])
    mixer_out = (partial[...] + other[...]).astype(BF16)
    x_mid = (tok[...].astype(F32) + mixer_out.astype(F32)).astype(BF16)
    moe_in = scale_rows(x_mid.astype(F32), gain)
    for i in range(2):
        xm[i] = x_mid[:, i * half : (i + 1) * half]
        moe[i] = moe_in[:, i * half : (i + 1) * half]
    rows = jnp.dot(p1, moe[t], preferred_element_type=F32)
    for i in range(NZ):
        send1[i] = rows[8 * i : 8 * i + 8].astype(BF16)

    for p in range(1, NZ):
        zd = lax.rem(z + ORDER[p], NZ)
        along_z(send1.at[zd], recv1.at[p], s1s, s1r.at[p], ORDER[p])
    recv1[0] = send1[z]
    weights = [
        remote(gate_ref.at[0, theirs], wg.at[:, lanes], w_ss.at[0], w_rs.at[0], partner),
        remote(up_ref.at[0, theirs], wu.at[:, lanes], w_ss.at[1], w_rs.at[1], partner),
        remote(down_ref.at[0, :, theirs], wd.at[lanes], w_ss.at[2], w_rs.at[2], partner),
    ]

    picks = 2 * NQ
    column = iota((picks, 128), 0)
    expand = one_hot(iota((picks, 128), 1) == lax.rem(column, 2) * NQ + column // 2)
    for p in range(NZ):
        if p:
            wait_for("choices", recvc.at[p], scr.at[p])
        choose = nt_dot(expand, recvc[p]).astype(BF16)
        if p:
            wait_for("hop1", recv1.at[p], s1r.at[p])
        picked = jnp.dot(choose, recv1[p], preferred_element_type=F32)
        send2[p] = picked.reshape(NQ, 2, half).astype(BF16)
        for i, (a, c) in enumerate(plane, 1):
            q = q_of(a, c)
            remote(send2.at[p, q], recv2.at[p, i], s2s, s2r.at[PASS_OF[p]], (z * NQ + q, t))
        recv2[p, 0] = send2[p, me_q]

    loads["rex"].wait()
    loads["rg"].wait()
    scores = hit * sigmoid(jnp.dot(moe_in, rex[...], preferred_element_type=F32))
    group_prob = sigmoid(jnp.sum(in_group * nt_dot(moe_in, rg[...]), axis=1, keepdims=True))
    route_weight = group_prob * scores / jnp.sum(scores, axis=1, keepdims=True)
    weighed = jnp.concatenate([route_weight * first, route_weight * (hit - first)], axis=1)
    weighed = split_dot(weighed, fold)
    high = weighed.astype(BF16)
    low = (weighed - high.astype(F32)).astype(BF16)
    sendm[...] = (
        jnp.dot(p1, high, preferred_element_type=F32) + jnp.dot(p1, low, preferred_element_type=F32)
    ).reshape(NZ, 8, 128)
    for p in range(1, NZ):
        zd = lax.rem(z + ORDER[p], NZ)
        along_z(sendm.at[zd], recvm.at[p], sms, smr, ORDER[p])
    recvm[0] = sendm[z]

    for copy in local:
        copy.wait()
    arrive("experts", weights)

    others_q = pl.ds(1, NQ - 1)
    def begin(b):
        low, high = PASSES[b]
        lines = pl.ds(low * picks, (high - low) * picks)
        wait_for("hop2", recv2.at[pl.ds(low, high - low), others_q], s2r.at[b])
        flat = recv2[low:high].astype(F32).reshape((high - low) * picks, half).astype(BF16)
        copies, parts = [], []
        for k, weight in enumerate((wg, wu)):
            parts.append(jnp.dot(flat, weight[...], preferred_element_type=F32))
            part[k, lines] = parts[k].astype(BF16)
            copies.append(remote(part.at[k, lines], partr.at[k, lines], ps, pr.at[b, k], partner))
        return copies, parts

    def finish(b, copies, parts):
        low, high = PASSES[b]
        group = pl.ds(low, high - low)
        lines = pl.ds(low * picks, (high - low) * picks)
        arrive("gate", [copies[0]])
        gate_sum = parts[0] + partr[0, lines].astype(F32)
        gated = gate_sum * sigmoid(gate_sum)
        arrive("up", [copies[1]])
        hidden = (gated * (parts[1] + partr[1, lines].astype(F32))).astype(BF16)
        result = jnp.dot(hidden, wd[...], preferred_element_type=F32)
        res[low:high] = result.reshape(high - low, NQ, 2, half).astype(BF16)
        for i, (a, c) in enumerate(plane, 1):
            q = q_of(-a, -c)
            remote(res.at[group, i], ret.at[group, me_q], s3s, s3r.at[b], (z * NQ + q, t))
        for p in range(low, high):
            ret[p, me_q] = res[p, 0]

    flying = []
    for b in range(len(PASSES)):
        flying.append((b, *begin(b)))
        if len(flying) > FLIGHT:
            finish(*flying.pop(0))
    for item in flying:
        finish(*item)

    wait_for("weights", recvm.at[pl.ds(1, NZ - 1)], smr)
    for b, (low, high) in enumerate(PASSES):
        count = high - low
        meta = recvm[low:high].reshape(8 * count, 128)
        meta_hi = meta.astype(BF16)
        meta_lo = (meta - meta_hi.astype(F32)).astype(BF16)
        own = iota((8 * count, picks * count), 0) // 8 == iota((8 * count, picks * count), 1) // picks
        weigh = []
        for half_meta in (meta_hi, meta_lo):
            spread = jnp.concatenate([nt_dot(half_meta, expand)] * count, axis=1)
            weigh.append(jnp.where(own, spread, 0.0).astype(BF16))
        wait_for("hop3", ret.at[pl.ds(low, count), others_q], s3r.at[b])
        results = ret[low:high].astype(F32).reshape(count * picks, half).astype(BF16)
        summed = jnp.dot(weigh[0], results, preferred_element_type=F32)
        summed += jnp.dot(weigh[1], results, preferred_element_type=F32)
        for p in range(low, high):
            comb[p] = summed[8 * (p - low) : 8 * (p - low) + 8].astype(BF16)
        for p in range(low, high):
            if p:
                along_z(comb.at[p], back.at[z], s4s, s4r, -ORDER[p])
    back[z] = comb[0]
    wait_for("hop4", back.at[pl.ds(1, NZ - 1)], s4r)
    sums = back[...].astype(F32).reshape(64, half).astype(BF16)
    moe_out = jnp.dot(p1t, sums, preferred_element_type=F32)
    out_ref[...] = (xm[t].astype(F32) + moe_out).astype(BF16)

    for copy in sent + weights:
        copy.wait_send()
    others = pl.ds(1, NZ - 1)
    for region, sem in (
        (sendc.at[others], scs), (send1.at[others], s1s), (sendm.at[others], sms), (comb.at[others], s4s),
        (send2.at[:, others_q], s2s), (part, ps), (res.at[:, others_q], s3s),
    ):
        wait_for("sent", region, sem)


def exchange(partial, tok, norm, rg, rex, routes, gate, up, down):
    seqs, half = tok.shape[0], tok.shape[1] // 2
    fh = gate.shape[2]
    hbm = pl.BlockSpec(memory_space=pl.ANY)
    dma = pltpu.SemaphoreType.DMA
    small = (partial, tok, norm, rg, rex, routes)
    by_half = pltpu.VMEM((2, seqs, half), BF16)
    by_z = pltpu.VMEM((NZ, 8, half), BF16)
    by_q = pltpu.VMEM((NZ, NQ, 2, half), BF16)
    parts = pltpu.VMEM((2, 2 * NZ * NQ, 2 * fh), BF16)
    passes = len(PASSES)
    return pl.pallas_call(
        exchange_kernel,
        out_shape=jax.ShapeDtypeStruct((seqs, half), BF16),
        in_specs=[hbm] * 9,
        out_specs=pl.BlockSpec(memory_space=pltpu.VMEM),
        scratch_shapes=[pltpu.VMEM(a.shape, a.dtype) for a in small]
        + [
            pltpu.VMEM(partial.shape, F32),
            by_half,
            by_half,
            pltpu.VMEM((half, 2 * fh), BF16),
            pltpu.VMEM((half, 2 * fh), BF16),
            pltpu.VMEM((2 * fh, half), BF16),
            pltpu.VMEM((NZ, 8, 128), BF16),
            pltpu.VMEM((NZ, 8, 128), BF16),
            by_z,
            by_z,
            pltpu.VMEM((NZ, 8, 128), F32),
            pltpu.VMEM((NZ, 8, 128), F32),
            by_q,
            by_q,
            parts,
            parts,
            by_q,
            by_q,
            by_z,
            by_z,
            dma((len(small),)),
            dma((3,)), dma((3,)), dma((3,)),
            dma((1,)), dma((1,)),
            dma, dma((NZ,)), dma, dma((NZ,)), dma, dma,
            dma, dma((passes,)),
            dma, dma((passes, 2)),
            dma, dma((passes,)),
            dma, dma,
        ],
        compiler_params=pltpu.CompilerParams(
            collective_id=0, has_side_effects=True, vmem_limit_bytes=67043328
        ),
    )(*small, gate, up, down)


def shards(
    tokens_in, state_in, norm_mix, w_recept, w_key, w_value, decay_down, decay_up, decay_base,
    iclr_down, iclr_up, iclr_base, key_scale, key_mix, w_out, norm_moe, router_group,
    router_expert, routes, expert_gate, expert_up, expert_down,
):
    partial_value, state_out = front(
        tokens_in, norm_mix, w_recept, w_key, w_value, decay_down.T, decay_up, decay_base,
        iclr_down.T, iclr_up, iclr_base, key_scale, key_mix, w_out, state_in,
    )
    layer_out = exchange(
        partial_value, tokens_in, norm_moe, router_group.T, router_expert, routes.T,
        expert_gate, expert_up, expert_down,
    )
    return (layer_out, state_out)


def solution(mesh):
    in_specs = (
        P("ep", None),
        P("ep", "tp", None, None),
        P(),
        P(None, "tp"),
        P(None, "tp"),
        P(None, "tp"),
        P(),
        P(None, "tp"),
        P("tp"),
        P(),
        P(None, "tp"),
        P("tp"),
        P("tp"),
        P("tp"),
        P("tp", None),
        P(),
        P(),
        P(),
        P("ep", None),
        P("ep", None, "tp"),
        P("ep", None, "tp"),
        P("ep", "tp", None),
    )
    out_specs = (P("ep", "tp"), P("ep", "tp", None, None))
    return jax.shard_map(shards, mesh=mesh, in_specs=in_specs, out_specs=out_specs, check_vma=False)
```

```python
import math

import jax
import jax.numpy as jnp
from jax import lax
from jax.experimental import pallas as pl
from jax.experimental.pallas import tpu as pltpu
from jax.sharding import PartitionSpec as P

MESH = pl.DeviceIdType.MESH
F32 = jnp.float32
BF16 = jnp.bfloat16
NZ, NY, NX = 8, 4, 4
NQ = NY * NX
ORDER = (0, 1, 7, 2, 6, 3, 5, 4)
PASSES = ((0, 2), (2, 4), (4, 6), (6, 8))
FLIGHT = 1
PASS_OF = tuple(k for k, (low, high) in enumerate(PASSES) for _ in range(low, high))


def iota(shape, dim):
    return lax.broadcasted_iota(jnp.int32, shape, dim)


def wait_for(name, region, sem):
    with jax.named_scope(name):
        pltpu.make_async_copy(region, region, sem).wait()


def arrive(name, copies):
    with jax.named_scope(name):
        for copy in copies:
            copy.wait_recv()


def one_hot(where):
    return jnp.where(where, 1.0, 0.0).astype(BF16)


def nt_dot(a, b):
    return lax.dot_general(a, b, (((1,), (1,)), ((), ())), preferred_element_type=F32)


def scale_rows(values32, gain):
    mean = jnp.mean(values32 * values32, axis=-1, keepdims=True)
    return (values32 * lax.rsqrt(mean + 1e-06) * gain).astype(BF16)


def sigmoid(u):
    return 1.0 / (1.0 + jnp.exp(-u))


def split_dot(a, b):
    hi = a.astype(BF16)
    lo = (a - hi.astype(F32)).astype(BF16)
    return jnp.dot(hi, b, preferred_element_type=F32) + jnp.dot(lo, b, preferred_element_type=F32)


def front_kernel(
    tok_ref, norm_ref, wr_ref, wk_ref, wv_ref, dd_ref, du_ref, db_ref, id_ref, iu_ref, ib_ref,
    ks_ref, km_ref, wo_ref, state_ref,
    partial_ref, state_out_ref,
    tok, norm, wr, wk, wv, dd, du, db, idn, iu, ib, ks, km, wo, sin, sout, lhs, decay, tall,
    isem, ssem, osem,
):
    seqs, heads, hs, _ = state_ref.shape
    width = heads * hs
    chunk = 8
    chunks = seqs // chunk
    loads = {}
    order = [
        ("tok", tok_ref, tok), ("norm", norm_ref, norm), ("wk", wk_ref, wk), ("dd", dd_ref, dd), ("id", id_ref, idn),
        ("wv", wv_ref, wv), ("wr", wr_ref, wr), ("du", du_ref, du), ("db", db_ref, db), ("iu", iu_ref, iu),
        ("ib", ib_ref, ib), ("ks", ks_ref, ks), ("km", km_ref, km),
    ]
    for i, (name, src, dst) in enumerate(order):
        loads[name] = pltpu.make_async_copy(src, dst, isem.at[i])
        loads[name].start()
    states = []
    for c in range(chunks):
        rows = pl.ds(c * chunk, chunk)
        states.append(pltpu.make_async_copy(state_ref.at[rows], sin.at[rows], ssem.at[c]))
        states[c].start()
    loads["wo"] = pltpu.make_async_copy(wo_ref, wo, isem.at[len(order)])
    loads["wo"].start()

    def got(*names):
        for name in names:
            loads[name].wait()

    got("tok", "norm")
    normed = scale_rows(tok[...].astype(F32), norm[...].astype(F32).reshape(1, -1))

    def project(weight):
        return jnp.dot(normed, weight[...], preferred_element_type=F32).astype(BF16)

    got("wk")
    key = project(wk).astype(F32)
    got("dd", "id")
    decay_low = jnp.tanh(nt_dot(normed, dd[...])).astype(BF16)
    iclr_low = nt_dot(normed, idn[...]).astype(BF16)
    got("wv", "wr")
    value = project(wv)
    recept = project(wr)
    got("du", "db", "iu", "ib", "ks", "km")
    rate_in = db[...].reshape(1, -1) + jnp.dot(decay_low, du[...], preferred_element_type=F32)
    decays = jnp.exp(-math.exp(-0.5) * sigmoid(rate_in))
    learn = sigmoid(ib[...].reshape(1, -1) + jnp.dot(iclr_low, iu[...], preferred_element_type=F32))
    scaled = key * ks[...].astype(F32).reshape(1, -1)
    head_ones = jnp.where(iota((width, width), 0) // hs == iota((width, width), 1) // hs, 1.0, 0.0).astype(BF16)
    unit_key = scaled * lax.rsqrt(split_dot(scaled * scaled, head_ones) + 1e-06)
    key_mod = key * (1.0 + (learn - 1.0) * km[...].astype(F32).reshape(1, -1))

    def by_head(values):
        return jnp.concatenate([values[:, h * hs : (h + 1) * hs] for h in range(heads)], axis=0)

    pairs = heads * seqs
    decay[...] = by_head(decays)
    keys_u = by_head(unit_key).astype(BF16)
    right = jnp.concatenate([by_head(-unit_key * learn), by_head(key_mod)], axis=0).astype(BF16)
    reads = by_head(recept.astype(F32)).astype(BF16)
    pick = jnp.where(iota((seqs, pairs), 0) == lax.rem(iota((seqs, pairs), 1), seqs), 1.0, 0.0).astype(BF16)
    spread = lax.dot_general(value, pick, (((0,), (0,)), ((), ())), preferred_element_type=F32).astype(BF16)

    lane = iota((hs, pairs), 1)
    tall[...] = jnp.zeros_like(tall)
    for c in range(chunks):
        states[c].wait()
        for s in range(c * chunk, (c + 1) * chunk):
            found = nt_dot(sin[s].reshape(width, hs).astype(BF16), keys_u)
            for h in range(heads):
                own = lane == h * seqs + s
                rows = slice(h * hs, (h + 1) * hs)
                lhs[s - c * chunk, rows, :pairs] = jnp.where(own, found[rows], 0.0).astype(BF16)
                lhs[s - c * chunk, rows, pairs:] = jnp.where(own, spread[rows], jnp.zeros((), BF16))
        for s in range(c * chunk, (c + 1) * chunk):
            update = jnp.dot(lhs[s - c * chunk], right, preferred_element_type=F32)
            for h in range(heads):
                row = h * seqs + s
                sout[s, h] = sin[s, h] * decay[row : row + 1, :] + update[h * hs : (h + 1) * hs]
        rows = pl.ds(c * chunk, chunk)
        pltpu.make_async_copy(sout.at[rows], state_out_ref.at[rows], osem.at[c]).start()
        for s in range(c * chunk, (c + 1) * chunk):
            seen = nt_dot(sout[s].reshape(width, hs).astype(BF16), reads)
            for h in range(heads):
                rows = slice(h * hs, (h + 1) * hs)
                tall[rows] = jnp.where(lane == h * seqs + s, seen[rows], tall[rows])
    mixed = nt_dot(pick, tall[...].astype(BF16)).astype(BF16)
    got("wo")
    partial_ref[...] = jnp.dot(mixed, wo[...], preferred_element_type=F32)
    for c in range(chunks):
        rows = pl.ds(c * chunk, chunk)
        pltpu.make_async_copy(sout.at[rows], state_out_ref.at[rows], osem.at[c]).wait()


def front(tok, norm, wr, wk, wv, dd, du, db, idn, iu, ib, ks, km, wo, state):
    seqs, heads, hs, _ = state.shape
    width, pairs = heads * hs, heads * seqs
    hbm = pl.BlockSpec(memory_space=pltpu.HBM)
    args = (tok, norm, wr, wk, wv, dd, du, db, idn, iu, ib, ks, km, wo)
    return pl.pallas_call(
        front_kernel,
        out_shape=(
            jax.ShapeDtypeStruct(tok.shape, F32),
            jax.ShapeDtypeStruct(state.shape, F32),
        ),
        in_specs=[hbm] * 15,
        out_specs=(pl.BlockSpec(memory_space=pltpu.VMEM), hbm),
        scratch_shapes=[pltpu.VMEM(a.shape, a.dtype) for a in args]
        + [
            pltpu.VMEM(state.shape, F32),
            pltpu.VMEM(state.shape, F32),
            pltpu.VMEM((8, width, 2 * pairs), BF16),
            pltpu.VMEM((pairs, hs), F32),
            pltpu.VMEM((width, pairs), F32),
            pltpu.SemaphoreType.DMA((len(args),)),
            pltpu.SemaphoreType.DMA((seqs // 8,)),
            pltpu.SemaphoreType.DMA((seqs // 8,)),
        ],
        compiler_params=pltpu.CompilerParams(vmem_limit_bytes=67043328),
    )(*args, state)


def exchange_kernel(
    partial_ref, tok_ref, norm_ref, rg_ref, re_ref, routes_ref, gate_ref, up_ref, down_ref,
    out_ref,
    partial, tok, norm, rg, rex, routes, other, xm, moe,
    wg, wu, wd, sendc, recvc, send1, recv1, sendm, recvm, send2, recv2, part, partr, res, ret, comb, back,
    isem, wsem, w_ss, w_rs, xs, xr, scs, scr, s1s, s1r, sms, smr, s2s, s2r, ps, pr, s3s, s3r, s4s, s4r,
):
    seqs, half = out_ref.shape
    fh = gate_ref.shape[2]
    experts = re_ref.shape[1]
    groups = rg_ref.shape[0]
    e = lax.axis_index("ep")
    t = lax.axis_index("tp")
    z, y, x = e // NQ, lax.rem(e // NX, NY), lax.rem(e, NX)
    me_q = lax.rem(e, NQ)
    partner = (e, 1 - t)

    def z_peer(d):
        return lax.rem(z + d + NZ, NZ) * NQ + me_q

    def q_of(a, b):
        return lax.rem(y + a + NY, NY) * NX + lax.rem(x + b + NX, NX)

    plane = [(a, b) for a in range(NY) for b in range(NX) if a or b]

    barrier = pltpu.get_barrier_semaphore()
    pl.semaphore_signal(barrier, inc=1, device_id=partner, device_id_type=MESH)
    for d in range(1, NZ):
        pl.semaphore_signal(barrier, inc=1, device_id=(z_peer(d), t), device_id_type=MESH)
    for a, b in plane:
        pl.semaphore_signal(barrier, inc=1, device_id=(z * NQ + q_of(a, b), t), device_id_type=MESH)

    mine = pl.ds(pl.multiple_of(t * half, half), half)
    theirs = pl.ds(pl.multiple_of((1 - t) * half, half), half)
    lanes = pl.ds(pl.multiple_of(t * fh, fh), fh)
    local = [
        pltpu.make_async_copy(gate_ref.at[0, mine], wg.at[:, lanes], wsem.at[0]),
        pltpu.make_async_copy(up_ref.at[0, mine], wu.at[:, lanes], wsem.at[1]),
        pltpu.make_async_copy(down_ref.at[0, :, mine], wd.at[lanes], wsem.at[2]),
    ]
    loads = {}
    for i, (name, src, dst) in enumerate([
        ("partial", partial_ref, partial), ("routes", routes_ref, routes), ("tok", tok_ref, tok), ("norm", norm_ref, norm),
        ("rex", re_ref, rex), ("rg", rg_ref, rg),
    ]):
        loads[name] = pltpu.make_async_copy(src, dst, isem.at[i])
        loads[name].start()
    for copy in local:
        copy.start()

    with jax.named_scope("enter"):
        loads["partial"].wait()
        pl.semaphore_wait(barrier, NZ + NQ - 1)

    def remote(src, dst, ss, rs, device):
        copy = pltpu.make_async_remote_copy(src, dst, ss, rs, device_id=device, device_id_type=MESH)
        copy.start()
        return copy

    def along_z(src, dst, ss, rs, step):
        return remote(src, dst, ss, rs, (z_peer(step), t))

    sent = [remote(partial, other, xs.at[0], xr.at[0], partner)]
    mixer_copy = sent[0]
    loads["routes"].wait()
    table = jnp.concatenate([routes[...].astype(F32), jnp.zeros_like(routes, F32)], axis=0).astype(BF16)
    named = nt_dot(one_hot(iota((seqs, seqs), 0) == iota((seqs, seqs), 1)), table)
    expert_lane = iota((seqs, experts), 1).astype(F32)
    hit = jnp.zeros((seqs, experts), F32)
    for k in range(routes.shape[0]):
        hit += jnp.where(named[:, k : k + 1] == expert_lane, 1.0, 0.0)
    earlier = one_hot(iota((seqs, seqs), 1) < iota((seqs, seqs), 0))
    first = jnp.where(jnp.dot(earlier, hit.astype(BF16), preferred_element_type=F32) < 0.5, hit, 0.0)
    fold_row = iota((2 * experts, 128), 0)
    fold = one_hot(iota((2 * experts, 128), 1) == (fold_row // experts) * NQ + lax.rem(fold_row, NQ))
    group_of = one_hot(iota((experts, groups), 0) // (experts // groups) == iota((experts, groups), 1))
    in_group = jnp.where(jnp.dot(hit.astype(BF16), group_of, preferred_element_type=F32) > 0.5, 1.0, 0.0)
    before = jnp.dot(earlier, in_group.astype(BF16), preferred_element_type=F32)
    slot = jnp.sum(in_group * (4.0 * iota((seqs, groups), 1).astype(F32) + before), axis=1, keepdims=True)
    p1t = one_hot(slot == iota((seqs, 64), 1).astype(F32))
    p1 = nt_dot(one_hot(iota((64, 64), 0) == iota((64, 64), 1)), p1t).astype(BF16)
    ranked = jnp.concatenate([first, hit - first], axis=1)
    choice = jnp.dot(ranked.astype(BF16), fold, preferred_element_type=F32).astype(BF16)
    choice = jnp.dot(p1, choice, preferred_element_type=F32)
    for i in range(NZ):
        sendc[i] = choice[8 * i : 8 * i + 8].astype(BF16)

    for p in range(1, NZ):
        zd = lax.rem(z + ORDER[p], NZ)
        along_z(sendc.at[zd], recvc.at[p], scs, scr.at[p], ORDER[p])
    recvc[0] = sendc[z]
    loads["tok"].wait()
    loads["norm"].wait()
    gain = norm[...].astype(F32).reshape(1, -1)
    arrive("mixer", [mixer_copy])
    mixer_out = (partial[...] + other[...]).astype(BF16)
    x_mid = (tok[...].astype(F32) + mixer_out.astype(F32)).astype(BF16)
    moe_in = scale_rows(x_mid.astype(F32), gain)
    for i in range(2):
        xm[i] = x_mid[:, i * half : (i + 1) * half]
        moe[i] = moe_in[:, i * half : (i + 1) * half]
    rows = jnp.dot(p1, moe[t], preferred_element_type=F32)
    for i in range(NZ):
        send1[i] = rows[8 * i : 8 * i + 8].astype(BF16)

    for p in range(1, NZ):
        zd = lax.rem(z + ORDER[p], NZ)
        along_z(send1.at[zd], recv1.at[p], s1s, s1r.at[p], ORDER[p])
    recv1[0] = send1[z]
    weights = [
        remote(gate_ref.at[0, theirs], wg.at[:, lanes], w_ss.at[0], w_rs.at[0], partner),
        remote(up_ref.at[0, theirs], wu.at[:, lanes], w_ss.at[1], w_rs.at[1], partner),
        remote(down_ref.at[0, :, theirs], wd.at[lanes], w_ss.at[2], w_rs.at[2], partner),
    ]

    picks = 2 * NQ
    column = iota((picks, 128), 0)
    expand = one_hot(iota((picks, 128), 1) == lax.rem(column, 2) * NQ + column // 2)
    for p in range(NZ):
        if p:
            wait_for("choices", recvc.at[p], scr.at[p])
        choose = nt_dot(expand, recvc[p]).astype(BF16)
        if p:
            wait_for("hop1", recv1.at[p], s1r.at[p])
        picked = jnp.dot(choose, recv1[p], preferred_element_type=F32)
        send2[p] = picked.reshape(NQ, 2, half).astype(BF16)
        for i, (a, c) in enumerate(plane, 1):
            q = q_of(a, c)
            remote(send2.at[p, q], recv2.at[p, i], s2s, s2r.at[PASS_OF[p]], (z * NQ + q, t))
        recv2[p, 0] = send2[p, me_q]

    loads["rex"].wait()
    loads["rg"].wait()
    scores = hit * sigmoid(jnp.dot(moe_in, rex[...], preferred_element_type=F32))
    group_prob = sigmoid(jnp.sum(in_group * nt_dot(moe_in, rg[...]), axis=1, keepdims=True))
    route_weight = group_prob * scores / jnp.sum(scores, axis=1, keepdims=True)
    weighed = jnp.concatenate([route_weight * first, route_weight * (hit - first)], axis=1)
    weighed = split_dot(weighed, fold)
    high = weighed.astype(BF16)
    low = (weighed - high.astype(F32)).astype(BF16)
    sendm[...] = (
        jnp.dot(p1, high, preferred_element_type=F32) + jnp.dot(p1, low, preferred_element_type=F32)
    ).reshape(NZ, 8, 128)
    for p in range(1, NZ):
        zd = lax.rem(z + ORDER[p], NZ)
        along_z(sendm.at[zd], recvm.at[p], sms, smr, ORDER[p])
    recvm[0] = sendm[z]

    for copy in local:
        copy.wait()
    arrive("experts", weights)

    others_q = pl.ds(1, NQ - 1)
    def begin(b):
        low, high = PASSES[b]
        lines = pl.ds(low * picks, (high - low) * picks)
        wait_for("hop2", recv2.at[pl.ds(low, high - low), others_q], s2r.at[b])
        flat = recv2[low:high].astype(F32).reshape((high - low) * picks, half).astype(BF16)
        copies, parts = [], []
        for k, weight in enumerate((wg, wu)):
            parts.append(jnp.dot(flat, weight[...], preferred_element_type=F32))
            part[k, lines] = parts[k].astype(BF16)
            copies.append(remote(part.at[k, lines], partr.at[k, lines], ps, pr.at[b, k], partner))
        return copies, parts

    def finish(b, copies, parts):
        low, high = PASSES[b]
        group = pl.ds(low, high - low)
        lines = pl.ds(low * picks, (high - low) * picks)
        arrive("gate", [copies[0]])
        gate_sum = parts[0] + partr[0, lines].astype(F32)
        gated = gate_sum * sigmoid(gate_sum)
        arrive("up", [copies[1]])
        hidden = (gated * (parts[1] + partr[1, lines].astype(F32))).astype(BF16)
        result = jnp.dot(hidden, wd[...], preferred_element_type=F32)
        res[low:high] = result.reshape(high - low, NQ, 2, half).astype(BF16)
        for i, (a, c) in enumerate(plane, 1):
            q = q_of(-a, -c)
            remote(res.at[group, i], ret.at[group, me_q], s3s, s3r.at[b], (z * NQ + q, t))
        for p in range(low, high):
            ret[p, me_q] = res[p, 0]

    flying = []
    for b in range(len(PASSES)):
        flying.append((b, *begin(b)))
        if len(flying) > FLIGHT:
            finish(*flying.pop(0))
    for item in flying:
        finish(*item)

    wait_for("weights", recvm.at[pl.ds(1, NZ - 1)], smr)
    for b, (low, high) in enumerate(PASSES):
        count = high - low
        meta = recvm[low:high].reshape(8 * count, 128)
        meta_hi = meta.astype(BF16)
        meta_lo = (meta - meta_hi.astype(F32)).astype(BF16)
        own = iota((8 * count, picks * count), 0) // 8 == iota((8 * count, picks * count), 1) // picks
        weigh = []
        for half_meta in (meta_hi, meta_lo):
            spread = jnp.concatenate([nt_dot(half_meta, expand)] * count, axis=1)
            weigh.append(jnp.where(own, spread, 0.0).astype(BF16))
        wait_for("hop3", ret.at[pl.ds(low, count), others_q], s3r.at[b])
        results = ret[low:high].astype(F32).reshape(count * picks, half).astype(BF16)
        summed = jnp.dot(weigh[0], results, preferred_element_type=F32)
        summed += jnp.dot(weigh[1], results, preferred_element_type=F32)
        for p in range(low, high):
            comb[p] = summed[8 * (p - low) : 8 * (p - low) + 8].astype(BF16)
        for p in range(low, high):
            if p:
                along_z(comb.at[p], back.at[z], s4s, s4r, -ORDER[p])
    back[z] = comb[0]
    wait_for("hop4", back.at[pl.ds(1, NZ - 1)], s4r)
    sums = back[...].astype(F32).reshape(64, half).astype(BF16)
    moe_out = jnp.dot(p1t, sums, preferred_element_type=F32)
    out_ref[...] = (xm[t].astype(F32) + moe_out).astype(BF16)

    for copy in sent + weights:
        copy.wait_send()
    others = pl.ds(1, NZ - 1)
    for region, sem in (
        (sendc.at[others], scs), (send1.at[others], s1s), (sendm.at[others], sms), (comb.at[others], s4s),
        (send2.at[:, others_q], s2s), (part, ps), (res.at[:, others_q], s3s),
    ):
        wait_for("sent", region, sem)


def exchange(partial, tok, norm, rg, rex, routes, gate, up, down):
    seqs, half = tok.shape[0], tok.shape[1] // 2
    fh = gate.shape[2]
    hbm = pl.BlockSpec(memory_space=pl.ANY)
    dma = pltpu.SemaphoreType.DMA
    small = (partial, tok, norm, rg, rex, routes)
    by_half = pltpu.VMEM((2, seqs, half), BF16)
    by_z = pltpu.VMEM((NZ, 8, half), BF16)
    by_q = pltpu.VMEM((NZ, NQ, 2, half), BF16)
    parts = pltpu.VMEM((2, 2 * NZ * NQ, 2 * fh), BF16)
    passes = len(PASSES)
    return pl.pallas_call(
        exchange_kernel,
        out_shape=jax.ShapeDtypeStruct((seqs, half), BF16),
        in_specs=[hbm] * 9,
        out_specs=pl.BlockSpec(memory_space=pltpu.VMEM),
        scratch_shapes=[pltpu.VMEM(a.shape, a.dtype) for a in small]
        + [
            pltpu.VMEM(partial.shape, F32),
            by_half,
            by_half,
            pltpu.VMEM((half, 2 * fh), BF16),
            pltpu.VMEM((half, 2 * fh), BF16),
            pltpu.VMEM((2 * fh, half), BF16),
            pltpu.VMEM((NZ, 8, 128), BF16),
            pltpu.VMEM((NZ, 8, 128), BF16),
            by_z,
            by_z,
            pltpu.VMEM((NZ, 8, 128), F32),
            pltpu.VMEM((NZ, 8, 128), F32),
            by_q,
            by_q,
            parts,
            parts,
            by_q,
            by_q,
            by_z,
            by_z,
            dma((len(small),)),
            dma((3,)), dma((3,)), dma((3,)),
            dma((1,)), dma((1,)),
            dma, dma((NZ,)), dma, dma((NZ,)), dma, dma,
            dma, dma((passes,)),
            dma, dma((passes, 2)),
            dma, dma((passes,)),
            dma, dma,
        ],
        compiler_params=pltpu.CompilerParams(
            collective_id=0, has_side_effects=True, vmem_limit_bytes=67043328
        ),
    )(*small, gate, up, down)


def shards(
    tokens_in, state_in, norm_mix, w_recept, w_key, w_value, decay_down, decay_up, decay_base,
    iclr_down, iclr_up, iclr_base, key_scale, key_mix, w_out, norm_moe, router_group,
    router_expert, routes, expert_gate, expert_up, expert_down,
):
    partial_value, state_out = front(
        tokens_in, norm_mix, w_recept, w_key, w_value, decay_down.T, decay_up, decay_base,
        iclr_down.T, iclr_up, iclr_base, key_scale, key_mix, w_out, state_in,
    )
    layer_out = exchange(
        partial_value, tokens_in, norm_moe, router_group.T, router_expert, routes.T,
        expert_gate, expert_up, expert_down,
    )
    return (layer_out, state_out)


def solution(mesh):
    in_specs = (
        P("ep", None),
        P("ep", "tp", None, None),
        P(),
        P(None, "tp"),
        P(None, "tp"),
        P(None, "tp"),
        P(),
        P(None, "tp"),
        P("tp"),
        P(),
        P(None, "tp"),
        P("tp"),
        P("tp"),
        P("tp"),
        P("tp", None),
        P(),
        P(),
        P(),
        P("ep", None),
        P("ep", None, "tp"),
        P("ep", None, "tp"),
        P("ep", "tp", None),
    )
    out_specs = (P("ep", "tp"), P("ep", "tp", None, None))
    return jax.shard_map(shards, mesh=mesh, in_specs=in_specs, out_specs=out_specs, check_vma=False)
```
